32 devices in a mesh: grp: 2 (over y), ep: 4 (over z), tp: 4 (over x, core).
Axes of the slice: x: 2, y: 2, z: 4, core: 2. Of those that a mesh axis runs over, the one named last changes fastest.
Arguments:
- queries: bfloat16 [4096, 768], P(('grp', 'ep'), 'tp'), parts along dimension 0, may hold values from -6 to 6
- key_value: bfloat16 [4096, 4, 128], P(('grp', 'ep'), 'tp'), parts along dimension 0, may hold values from -6 to 6
- key_bias: bfloat16 [4, 4096], P('tp', ('grp', 'ep')), parts along dimension 1, may hold values from -20 to 0
- out_weight: bfloat16 [768, 2048], P('tp'), may hold values from -0.75 to 0.75
- expert_input: bfloat16 [4096, 2048], P(('grp', 'ep', 'tp')), parts along dimension 0, may hold values from -6 to 6
- norm_gain: float32 [2048], replicated, may hold values from 0.1 to 1.9
- routes: int32 [4096, 4], P(('grp', 'ep', 'tp')), parts along dimension 0, may hold values from 0 to 15, as said below
- route_weights: float32 [4096, 4], P(('grp', 'ep', 'tp')), parts along dimension 0, may hold values from 0.2 to 1
- gate_weight: bfloat16 [16, 2048, 512], P(('ep', 'tp')), may hold values from -0.125 to 0.125
- up_weight: bfloat16 [16, 2048, 512], P(('ep', 'tp')), may hold values from -0.125 to 0.125
- down_weight: bfloat16 [16, 512, 2048], P(('ep', 'tp')), may hold values from -0.25 to 0.25
- shared_gate: bfloat16 [2048, 256], replicated, may hold values from -0.125 to 0.125
- shared_up: bfloat16 [2048, 256], replicated, may hold values from -0.125 to 0.125
- shared_down: bfloat16 [256, 2048], replicated, may hold values from -0.375 to 0.375
Outputs:
- mixer_output: bfloat16 [4096, 2048], P(('grp', 'ep', 'tp')), parts along dimension 0
- expert_output: bfloat16 [4096, 2048], P(('grp', 'ep', 'tp')), parts along dimension 0
The draws below stay inside these ranges and needn't reach their ends.
There are 2 independent parts, one for each index of `grp`. The reference program is written for one: setup_inputs(seed, part) draws one part's arguments, and reference() takes and returns one part's arrays. A program takes and returns all parts, laid end to end along the dimension named above; an argument that names none is the same for every part. Nothing has to cross between parts.
Inputs may be any that keep to these rules, and one draw needn't show every extreme that they name: `routes`: each row names 4 different experts. Among the 128 rows of one device no expert is named more than 48 times, and in every draw one expert is named exactly 48 times in the rows of every device.
All inputs are finite; a program needn't handle non-finite values.
Results may differ from the reference program's by a relative error of at most 0.009.
Values may be sent and summed in bfloat16 or wider, within the bound.
A program may use at most 128 MiB of HBM per device.

```python
import math
import jax
import jax.numpy as jnp
import numpy as np
from jax import lax

D = 2048
HD = 64
HEADS = 12
KEY_HEAD_COUNT = 4
EFF = 512
SFF = 256
TOPK = 4
TOK = 128
SPAN = 512
DEVSEQ = 4
SEQUENCE_LENGTH = 2048
TOTAL_POSITIONS = 2048
TOKENS = 2048
EXPERTS = 16
CAP = 48
HOT = 2
N_TP = 4


def draw_routes(key, part):
    key_hot = jax.random.fold_in(key, 11)
    key_order = jax.random.fold_in(key, 12)
    key_rows = jax.random.fold_in(key, 13)
    sources = TOKENS // TOK
    hot_expert = jax.random.randint(key_hot, (), 0, EXPERTS, dtype=jnp.int32)
    ordinal = jnp.broadcast_to(jnp.arange(EXPERTS, dtype=jnp.int32), (sources, EXPERTS))
    orders = jax.random.permutation(key_order, ordinal, axis=1, independent=True)
    hot_place = jnp.argmax(orders == hot_expert, axis=1)
    columns = jnp.arange(EXPERTS, dtype=jnp.int32)[None, :]
    leading = orders[:, :1]
    orders = jnp.where(columns == 0, hot_expert, jnp.where(columns == hot_place[:, None], leading, orders))
    remaining = TOK * TOPK - HOT * CAP
    others = EXPERTS - HOT
    counts = np.array([CAP] * HOT + [remaining // others + (1 if index < remaining % others else 0) for index in range(others)])
    rank_list = np.repeat(np.arange(EXPERTS), counts)
    tickets = orders[:, rank_list]
    laid_out = jnp.transpose(tickets.reshape(sources, TOPK, TOK), (0, 2, 1))
    row_ordinal = jnp.broadcast_to(jnp.arange(TOK, dtype=jnp.int32), (sources, TOK))
    row_orders = jax.random.permutation(key_rows, row_ordinal, axis=1, independent=True)
    shuffled = jnp.take_along_axis(laid_out, jnp.broadcast_to(row_orders[:, :, None], laid_out.shape), axis=1)
    return shuffled.reshape(TOKENS, TOPK).astype(jnp.int32)


def draw_key_bias(key, part):
    ranking = jax.random.permutation(jax.random.fold_in(key, 21), KEY_HEAD_COUNT)
    fast_count = KEY_HEAD_COUNT // 2
    is_fast = ranking < fast_count
    drawn_version = jnp.where(is_fast, -jnp.log(40.0), -jnp.log(float(SEQUENCE_LENGTH)) - 1.0)[:, None]
    jaggedness = jax.random.uniform(jax.random.fold_in(key, 22), (KEY_HEAD_COUNT, TOTAL_POSITIONS), jnp.float32, -0.5, 0.5)
    block_by_block = jax.random.uniform(jax.random.fold_in(key, 23), (KEY_HEAD_COUNT, TOTAL_POSITIONS // SPAN), jnp.float32, -0.7, 0.7)
    block_by_block = jnp.repeat(block_by_block, SPAN, axis=1)
    spike_events = jax.random.randint(jax.random.fold_in(key, 24), (KEY_HEAD_COUNT, TOTAL_POSITIONS), 0, SEQUENCE_LENGTH) < 3
    spike_height = jax.random.uniform(jax.random.fold_in(key, 25), (KEY_HEAD_COUNT, TOTAL_POSITIONS), jnp.float32, -1.2, -0.3)
    return jnp.where(spike_events, spike_height, drawn_version + jaggedness + block_by_block).astype(jnp.bfloat16)


def level_of(stream_key, extent, split, smallest, high):
    gain, own = 1.0, jax.random.fold_in(stream_key, 6)
    for dim, blocks in split:
        heights = jnp.exp(jax.random.uniform(jax.random.fold_in(own, dim), (blocks,), jnp.float32, smallest / len(split), high / len(split)))
        gain = gain * jnp.repeat(heights, extent[dim] // blocks).reshape([-1 if axis == dim else 1 for axis in range(len(extent))])
    return gain


def gaussian(key, shape, spread, limit, shards=(), kind=jnp.bfloat16):
    drawn = spread * jax.random.normal(key, shape, jnp.float32)
    if shards:
        drawn = drawn * level_of(key, shape, shards, -0.22, 0.18)
    return jnp.clip(drawn, -limit, limit).astype(kind)


def setup_inputs(seed: int = 0, part: int = 0) -> dict:
    keys = jax.random.split(jax.random.key(seed), 15)
    part_splits = jax.random.split(jax.random.fold_in(keys[14], part), 15)
    return {
        "queries": gaussian(part_splits[0], (TOTAL_POSITIONS, HEADS * HD), 1.0, 6.0, ((0, 4), (1, 4))),
        "key_value": gaussian(part_splits[1], (TOTAL_POSITIONS, KEY_HEAD_COUNT, 2 * HD), 1.0, 6.0, ((0, 4), (1, 4))),
        "key_bias": draw_key_bias(jax.random.fold_in(jax.random.fold_in(keys[14], part), 71), part),
        "out_weight": gaussian(keys[3], (HEADS * HD, D), HD ** -0.5, 0.75, ((0, 4),)),
        "expert_input": gaussian(part_splits[4], (TOKENS, D), 1.0, 6.0, ((0, 16),)),
        "norm_gain": jnp.clip(1.0 + 0.18 * jax.random.normal(keys[5], (D,), jnp.float32), 0.1, 1.9),
        "routes": draw_routes(jax.random.fold_in(jax.random.fold_in(keys[14], part), 71), part),
        "route_weights": jnp.clip(jnp.exp(math.log(1.0) - 1.609438 * jax.random.uniform(part_splits[7], (TOKENS, TOPK), jnp.float32) ** level_of(part_splits[7], (TOKENS, TOPK), ((0, 16),), -0.2, 0.2)), 0.2, 1.0),
        "gate_weight": gaussian(keys[8], (EXPERTS, D, EFF), D ** -0.5, 0.125, ((0, 16),)),
        "up_weight": gaussian(keys[9], (EXPERTS, D, EFF), D ** -0.5, 0.125, ((0, 16),)),
        "down_weight": gaussian(keys[10], (EXPERTS, EFF, D), EFF ** -0.5, 0.25, ((0, 16),)),
        "shared_gate": gaussian(keys[11], (D, SFF), D ** -0.5, 0.125),
        "shared_up": gaussian(keys[12], (D, SFF), D ** -0.5, 0.125),
        "shared_down": gaussian(keys[13], (SFF, D), SFF ** -0.5, 0.375),
    }


def piece_update(running, query_rows, key_rows, value_rows, key_offset, allowed):
    totals, kept_sum = running
    logits = jnp.einsum('sgrd,kgd->grsk', query_rows.astype(jnp.float32), key_rows.astype(jnp.float32)) * 0.125
    logits = logits + key_offset.astype(jnp.float32)[:, None, None, :]
    log_keep = jnp.where(allowed, -jax.nn.softplus(logits), 0.0)
    log_after = lax.cumsum(log_keep, axis=3, reverse=True) - log_keep
    weights = jnp.where(allowed, jnp.exp(jax.nn.log_sigmoid(logits) + log_after + kept_sum[..., None]), 0.0)
    weights = weights.astype(jnp.bfloat16)
    totals = totals + jnp.einsum('grsk,kgd->grsd', weights.astype(jnp.float32), value_rows.astype(jnp.float32))
    return (totals, kept_sum + lax.optimization_barrier(jnp.sum(log_keep, axis=3)))

def mixer_reference(queries, key_value, key_bias, out_weight):
    per_group = HEADS // KEY_HEAD_COUNT
    block_count = TOTAL_POSITIONS // SPAN
    query_blocks = queries.reshape(block_count, SPAN, KEY_HEAD_COUNT, per_group, HD)
    key_blocks = key_value[..., :HD].reshape(block_count, SPAN, KEY_HEAD_COUNT, HD)
    value_blocks = key_value[..., HD:].reshape(block_count, SPAN, KEY_HEAD_COUNT, HD)
    bias_blocks = jnp.transpose(key_bias.reshape(KEY_HEAD_COUNT, block_count, SPAN), (1, 0, 2))
    positions = jnp.arange(SPAN, dtype=jnp.int32)
    strict_mask = positions[None, :] < positions[:, None]
    full_mask = jnp.ones((SPAN, SPAN), dtype=bool)

    def one_block(block_index):
        query_rows = query_blocks[block_index]
        initial = (jnp.zeros((KEY_HEAD_COUNT, per_group, SPAN, HD), jnp.float32), jnp.zeros((KEY_HEAD_COUNT, per_group, SPAN), jnp.float32))
        running = piece_update(initial, query_rows, key_blocks[block_index], value_blocks[block_index], bias_blocks[block_index], strict_mask)

        def advance(distance, current):
            source = block_index - distance
            return piece_update(current, query_rows, key_blocks[source], value_blocks[source], bias_blocks[source], full_mask)
        chain_place = jnp.minimum((block_index + 2) % DEVSEQ, block_index)
        running = lax.fori_loop(1, chain_place + 1, advance, running)
        return running[0].astype(jnp.bfloat16)
    attended = lax.map(one_block, jnp.arange(block_count, dtype=jnp.int32))
    weight_blocks = out_weight.reshape(KEY_HEAD_COUNT, per_group, HD, D)
    group_heads = KEY_HEAD_COUNT // N_TP
    summed = jnp.zeros((block_count, SPAN, D), jnp.float32)
    for group_index in range(N_TP):
        part_rows = attended[:, group_index * group_heads:(group_index + 1) * group_heads].astype(jnp.float32)
        part_weight = weight_blocks[group_index * group_heads:(group_index + 1) * group_heads].astype(jnp.float32)
        group_terms = jnp.einsum('bgrsd,grde->bse', part_rows, part_weight).astype(jnp.bfloat16)
        summed = summed + group_terms.astype(jnp.float32)
    return summed.reshape(TOTAL_POSITIONS, D).astype(jnp.bfloat16)

def experts_reference(expert_input, norm_gain, routes, route_weights, gate_weight, up_weight, down_weight, shared_gate, shared_up, shared_down):
    widened = expert_input.astype(jnp.float32)
    normed = (widened * lax.rsqrt(lax.optimization_barrier(jnp.mean(widened * widened, axis=-1, keepdims=True)) + 1e-06) * norm_gain).astype(jnp.bfloat16)
    sources = TOKENS // TOK
    pair_count = TOK * TOPK
    block_routes = routes.reshape(sources, pair_count)
    one_hot = (block_routes[..., None] == jnp.arange(EXPERTS, dtype=jnp.int32)).astype(jnp.int32)
    slot_index = lax.optimization_barrier(jnp.sum((jnp.cumsum(one_hot, axis=1) - one_hot) * one_hot, axis=2))
    placing = (block_routes * sources + jnp.arange(sources, dtype=jnp.int32)[:, None]) * CAP + slot_index
    empty_pair = TOKENS * TOPK
    table = jnp.full((EXPERTS * sources * CAP,), empty_pair, jnp.int32)
    table = table.at[placing.reshape(-1)].set(jnp.arange(empty_pair, dtype=jnp.int32))
    table = table.reshape(EXPERTS, sources * CAP)
    padded_rows = jnp.concatenate([normed, jnp.zeros((1, D), jnp.bfloat16)], axis=0)
    padded_weights = jnp.concatenate([route_weights.reshape(-1), jnp.zeros((1,), jnp.float32)], axis=0)

    def expert_step(accumulated, inputs):
        picks, gate_one, up_one, down_one = inputs
        owners = picks // TOPK
        chosen = padded_rows[owners]
        gate_part = jnp.dot(chosen, gate_one, preferred_element_type=jnp.float32)
        up_part = jnp.dot(chosen, up_one, preferred_element_type=jnp.float32)
        hidden = (jax.nn.silu(gate_part) * up_part).astype(jnp.bfloat16)
        result = jnp.dot(hidden, down_one, preferred_element_type=jnp.float32).astype(jnp.bfloat16)
        scaled = result.astype(jnp.float32) * padded_weights[picks][:, None]
        return (accumulated.at[owners].add(scaled, mode='drop'), None)
    routed, _ = lax.scan(expert_step, jnp.zeros((TOKENS, D), jnp.float32), (table, gate_weight, up_weight, down_weight))
    shared_hidden = (jax.nn.silu(jnp.dot(normed, shared_gate, preferred_element_type=jnp.float32)) * jnp.dot(normed, shared_up, preferred_element_type=jnp.float32)).astype(jnp.bfloat16)
    shared_term = jnp.dot(shared_hidden, shared_down, preferred_element_type=jnp.float32)
    return (routed + shared_term).astype(jnp.bfloat16)

def reference(queries, key_value, key_bias, out_weight, expert_input, norm_gain, routes, route_weights, gate_weight, up_weight, down_weight, shared_gate, shared_up, shared_down):
    mixer_output = mixer_reference(queries, key_value, key_bias, out_weight)
    expert_output = experts_reference(expert_input, norm_gain, routes, route_weights, gate_weight, up_weight, down_weight, shared_gate, shared_up, shared_down)
    return (mixer_output, expert_output)
```

```python
import jax
import jax.numpy as jnp
from jax import lax
from jax.experimental import pallas as pl
from jax.experimental.pallas import tpu as pltpu
from jax.sharding import PartitionSpec as P

MESH = pl.DeviceIdType.MESH
F32 = jnp.float32
BF16 = jnp.bfloat16


def passed_along(block, axis, distance):
    devices = range(lax.axis_size(axis))
    route = [(i - distance, i) for i in devices if i - distance in devices]
    return lax.ppermute(block, axis, route)


def furthest_place(axis_size):
    chain_length = axis_size // max(1, axis_size // 4)
    return max(min((p + 2) % chain_length, p) for p in range(axis_size))


def attention_tile(q, k, v, bias, upper, kept, masked):
    z = lax.dot_general(q, k, (((1,), (1,)), ((), ())), preferred_element_type=F32) * 0.125 + bias
    tail = jnp.log(1.0 + jnp.exp(-jnp.abs(z)))
    log_sig = jnp.minimum(z, 0.0) - tail
    keep = -(jnp.maximum(z, 0.0) + tail)
    if masked:
        rows = lax.broadcasted_iota(jnp.int32, z.shape, 0)
        columns = lax.broadcasted_iota(jnp.int32, z.shape, 1)
        allowed = columns < rows
        keep = jnp.where(allowed, keep, 0.0)
    high = keep.astype(BF16)
    low = (keep - high.astype(F32)).astype(BF16)
    after = jnp.dot(high, upper, preferred_element_type=F32)
    after = after + jnp.dot(low, upper, preferred_element_type=F32)
    weight = jnp.exp(log_sig + after + kept)
    if masked:
        weight = jnp.where(allowed, weight, 0.0)
    part = jnp.dot(weight.astype(BF16), v, preferred_element_type=F32)
    return part, kept + jnp.sum(keep, axis=1, keepdims=True)


def attention_kernel(place_ref, q_ref, kv_ref, bias_ref, out_ref, total, kept):
    span, head_dim = q_ref.shape[1:]
    spans = kv_ref.shape[0]
    size = min(span, 256)
    tiles = span // size
    rows = lax.broadcasted_iota(jnp.int32, (size, size), 0)
    columns = lax.broadcasted_iota(jnp.int32, (size, size), 1)
    upper = jnp.where(rows > columns, 1.0, 0.0).astype(BF16)

    def tile(distance, i, j, masked, state):
        there = pl.ds(j * size, size)
        part, after = attention_tile(
            q_ref[0, i * size : (i + 1) * size, :],
            kv_ref[distance, 0, there, :head_dim],
            kv_ref[distance, 0, there, head_dim:],
            bias_ref[distance, 0, :, there].astype(F32),
            upper,
            state[1],
            masked,
        )
        return state[0] + part, after

    for i in range(tiles):
        state = (jnp.zeros((size, head_dim), F32), jnp.zeros((size, 1), F32))
        for j in range(i, -1, -1):
            state = tile(0, i, j, j == i, state)
        total[i] = state[0]
        kept[i] = jnp.broadcast_to(state[1], kept.shape[1:])
    for distance in range(1, spans):

        @pl.when(distance <= place_ref[0])
        def _():
            for i in range(tiles):
                state = (total[i], kept[i, :, :1])
                for j in range(tiles - 1, -1, -1):
                    state = tile(distance, i, j, False, state)
                total[i] = state[0]
                kept[i] = jnp.broadcast_to(state[1], kept.shape[1:])

    for i in range(tiles):
        out_ref[0, i * size : (i + 1) * size, :] = total[i].astype(out_ref.dtype)


def attend(queries, key_value, key_bias):
    span, key_groups, pair_width = key_value.shape
    head_dim = pair_width // 2
    heads = queries.shape[1] // head_dim
    per_group = heads // key_groups
    axis_size = lax.axis_size("ep")
    chain_length = axis_size // max(1, axis_size // 4)
    place = lax.axis_index("ep")
    chain_place = jnp.minimum((place + 2) % chain_length, place)
    furthest = furthest_place(axis_size)
    packed = jnp.concatenate([key_value.reshape(-1, pair_width), key_bias.reshape(-1, pair_width)])
    visiting = [packed]
    for _ in range(furthest):
        visiting.append(passed_along(visiting[-1], "ep", 1))
    visiting = jnp.stack(visiting)
    keys = visiting[:, : span * key_groups].reshape(-1, span, key_groups, pair_width)
    keys = keys.transpose(0, 2, 1, 3)
    biases = visiting[:, span * key_groups :].reshape(-1, key_groups, 1, span)
    size = min(span, 256)
    attended = pl.pallas_call(
        attention_kernel,
        grid=(heads,),
        out_shape=jax.ShapeDtypeStruct((heads, span, head_dim), BF16),
        in_specs=[
            pl.BlockSpec(memory_space=pltpu.SMEM),
            pl.BlockSpec((1, span, head_dim), lambda h: (h, 0, 0)),
            pl.BlockSpec((furthest + 1, 1, span, pair_width), lambda h: (0, h // per_group, 0, 0)),
            pl.BlockSpec((furthest + 1, 1, 1, span), lambda h: (0, h // per_group, 0, 0)),
        ],
        out_specs=pl.BlockSpec((1, span, head_dim), lambda h: (h, 0, 0)),
        scratch_shapes=[
            pltpu.VMEM((span // size, size, head_dim), F32),
            pltpu.VMEM((span // size, size, 128), F32),
        ],
        name="attention",
        cost_estimate=pl.CostEstimate(flops=4 * 10**9, bytes_accessed=10**6, transcendentals=0),
    )(
        chain_place.reshape(1),
        queries.reshape(span, heads, head_dim).transpose(1, 0, 2),
        keys,
        biases,
    )
    return attended.transpose(1, 0, 2).reshape(span, heads * head_dim)


def project(attended, out_weight):
    return jnp.dot(attended, out_weight, preferred_element_type=F32).astype(BF16)


def layer_kernel(
    capacity,
    q_ref,
    kv_ref,
    bias_ref,
    x_ref,
    gain_ref,
    routes_ref,
    route_weights_ref,
    out_weight_hbm,
    shared_gate_hbm,
    shared_up_hbm,
    shared_down_hbm,
    gate_hbm,
    up_hbm,
    down_hbm,
    mixer_ref,
    expert_ref,
    gathered,
    gathered_s,
    meta_out,
    meta,
    staged,
    staged_s,
    chosen,
    rows_in,
    rows_in_s,
    sums,
    sums_s,
    line_in,
    line_in_s,
    acc,
    acc_s,
    from_side,
    shared,
    out_weight_v,
    shared_gate_v,
    shared_up_v,
    shared_down_v,
    gate_v,
    up_v,
    down_v,
    kv_next,
    bias_row,
    bias_next,
    values_t,
    biases_t,
    att_total,
    att_kept,
    attended_t,
    terms,
    mixer_in,
    mixer_sum,
    mixer_side,
    load_sem,
    meta_send,
    meta_recv,
    kv_send,
    kv_recv,
    zs_send,
    zs_recv,
    s_send,
    s_recv,
    xa_send,
    xa_recv,
    xr_send,
    xr_recv,
    rz_send,
    rz_recv,
    last_send,
    last_recv,
    m_send,
    m_recv,
):
    count = lax.axis_size("ep")
    tokens, width = x_ref.shape
    columns = piece_columns(width)
    pieces = len(columns)
    cut = columns[0].stop
    items = pieces + 1
    z = lax.axis_index("ep")
    t = lax.axis_index("tp")
    x, c = t // 2, t % 2
    ox, oc = 1 - x, 1 - c
    places = (t, x * 2 + oc, ox * 2 + c, ox * 2 + oc)
    sibling, side = places[1], places[2]
    is_end = (z == 0) | (z == count - 1)

    def inside(zz):
        return (zz >= 0) & (zz < count)

    def copy(src, dst, send, recv, ep, tp):
        return pltpu.make_async_remote_copy(
            src_ref=src,
            dst_ref=dst,
            send_sem=send,
            recv_sem=recv,
            device_id={"ep": ep, "tp": tp},
            device_id_type=MESH,
        )

    def band(r):
        return slice(r * capacity, (r + 1) * capacity)

    loads = {
        name: pltpu.make_async_copy(a, b, load_sem.at[i])
        for i, (name, a, b) in enumerate(
            (
                ("shared_gate", shared_gate_hbm, shared_gate_v),
                ("shared_up", shared_up_hbm, shared_up_v),
                ("shared_down", shared_down_hbm, shared_down_v),
                ("gate", gate_hbm, gate_v),
                ("up", up_hbm, up_v),
                ("down", down_hbm, down_v),
                ("out_weight", out_weight_hbm, out_weight_v),
            )
        )
    }

    barrier = pltpu.get_barrier_semaphore()

    def greet(ep, tp):
        pl.semaphore_signal(barrier, 1, device_id={"ep": ep, "tp": tp}, device_id_type=MESH)

    for step in range(1, count):
        for sx in (0, 2):
            greet((z + step) % count, places[sx])
    for r in (1, 2, 3):
        greet(z, places[r])

    @pl.loop(0, tokens // 16)
    def _(block):
        rows = pl.ds(pl.multiple_of(block * 16, 16), 16)
        wide = x_ref[rows, :].astype(F32)
        mean = jnp.mean(wide * wide, axis=-1, keepdims=True)
        gathered[z, rows, :] = (wide * lax.rsqrt(mean + 1e-06) * gain_ref[...]).astype(BF16)

    lines = lax.broadcasted_iota(jnp.int32, (count * 8, tokens), 0)
    expert = (lines // 8) * 4 + lines % 4
    named = jnp.zeros((count * 8, tokens), F32)
    weight = jnp.zeros((count * 8, tokens), F32)
    for k in range(routes_ref.shape[0]):
        hit = routes_ref[k : k + 1, :] == expert
        named = named + jnp.where(hit, 1.0, 0.0)
        weight = weight + jnp.where(hit, route_weights_ref[k : k + 1, :], 0.0)
    before = lax.broadcasted_iota(jnp.int32, (tokens, tokens), 0) < lax.broadcasted_iota(
        jnp.int32, (tokens, tokens), 1
    )
    slot = jnp.dot(
        named.astype(BF16), jnp.where(before, 1.0, 0.0).astype(BF16), preferred_element_type=F32
    )
    slot = jnp.where(named > 0.5, slot, -1.0)
    meta_out[...] = jnp.where(lines % 8 < 4, slot, weight).reshape(meta_out.shape)
    meta[0, z] = meta_out[z]
    bias_row[...] = jnp.broadcast_to(bias_ref[...].astype(F32), bias_row.shape)

    pl.semaphore_wait(barrier, 2 * (count - 1) + 3)

    def meta_copy(step, sx):
        other = (z + step) % count
        return copy(
            meta_out.at[other],
            meta.at[sx, z],
            meta_send.at[sx, step],
            meta_recv.at[sx, z],
            other,
            places[2 * sx],
        )

    def meta_wait(sx, zz):
        copy(
            meta_out.at[zz], meta.at[sx, zz], meta_send.at[sx, 0], meta_recv.at[sx, zz], z, side
        ).wait_recv()

    def s_move():
        return copy(
            gathered.at[z, :, columns[0]], gathered_s.at[z], s_send.at[0], s_recv.at[0], z, side
        )

    def line(i, zz, item):
        block = gathered_s.at[zz] if item == pieces else gathered.at[zz, :, columns[item]]
        return copy(
            block, block, zs_send.at[i, item, zz], zs_recv.at[item, zz], z + 2 * i - 1, t
        )

    def kv_move(which):
        pair = ((kv_ref, kv_next), (bias_row, bias_next))[which]
        return copy(*pair, kv_send.at[which], kv_recv.at[which], z + 1, t)

    chain = count // max(1, count // 4)

    def chain_place(zz):
        return jnp.minimum((zz + 2) % chain, zz)

    sends_kv = (z + 1 < count) & (chain_place(z + 1) >= 1)
    takes_kv = chain_place(z) >= 1

    for step in range(1, count):
        for sx in range(2):
            meta_copy(step, sx).start()
    meta_copy(0, 1).start()
    s_move().start()
    for item in range(pieces):
        for i in range(2):

            @pl.when(inside(z + 2 * i - 1))
            def _():
                line(i, z, item).start()

    slots = lax.broadcasted_iota(jnp.int32, (capacity, tokens), 0).astype(F32)

    def one_hot(sx, zz, rels):
        return jnp.concatenate(
            [jnp.where(meta[sx, zz, pl.ds(places[r], 1), :] == slots, 1.0, 0.0) for r in rels],
            axis=0,
        ).astype(BF16)

    def spreader(sx, zz, rels):
        weights = jnp.concatenate(
            [
                jnp.where(
                    meta[sx, zz, pl.ds(places[r], 1), :] == slots,
                    meta[sx, zz, pl.ds(4 + places[r], 1), :],
                    0.0,
                )
                for r in rels
            ],
            axis=0,
        )
        high = weights.astype(BF16)
        return high, (weights - high.astype(F32)).astype(BF16)

    def spread(pair, rows):
        return sum(
            lax.dot_general(half, rows, (((0,), (0,)), ((), ())), preferred_element_type=F32)
            for half in pair
        )

    def row_copy(r, zz, p):
        if p == 0 and r == 3:
            return copy(
                staged_s.at[zz],
                chosen.at[zz, band(3), columns[0]],
                xa_send.at[r, p, zz],
                xa_recv.at[r, p, zz],
                z,
                sibling,
            )
        return copy(
            staged.at[zz, band(r - 1), columns[p]],
            chosen.at[zz, band(r), columns[p]],
            xa_send.at[r, p, zz],
            xa_recv.at[r, p, zz],
            z,
            places[r],
        )

    def pick(zz, p):
        rels = (0, 1) if p == 0 else (0, 1, 2, 3)
        picked = jnp.dot(
            one_hot(0, zz, rels), gathered[zz, :, columns[p]], preferred_element_type=F32
        ).astype(BF16)
        staged[zz, : (len(rels) - 1) * capacity, columns[p]] = picked[capacity:]
        chosen[zz, band(0), columns[p]] = picked[:capacity]
        for r in rels[:0:-1]:
            row_copy(r, zz, p).start()

    def pick_s(zz):
        picked = jnp.dot(
            one_hot(1, zz, (0, 1)), gathered_s[zz], preferred_element_type=F32
        ).astype(BF16)
        staged_s[zz] = picked[capacity:]
        chosen[zz, band(2), columns[0]] = picked[:capacity]
        row_copy(3, zz, 0).start()

    for p in (*range(1, pieces), 0):
        pick(z, p)
    s_move().wait_recv()
    for i in range(2):

        @pl.when(inside(z + 2 * i - 1))
        def _():
            line(i, z, pieces).start()

    @pl.when(sends_kv)
    def _():
        kv_move(1).start()
        kv_move(0).start()

    for load in loads.values():
        load.start()
    meta_wait(1, z)
    pick_s(z)

    span = kv_ref.shape[0]
    head_dim = kv_ref.shape[1] // 2
    heads = q_ref.shape[0] // head_dim
    size = min(span, 256)
    tiles = span // size
    key_line = lax.broadcasted_iota(jnp.int32, (size, size), 0)
    query_line = lax.broadcasted_iota(jnp.int32, (size, size), 1)

    def prepare(b, kv, bias):
        values_t[b] = kv[...].astype(F32).T[head_dim:, :].astype(BF16)
        biases_t[b] = jnp.broadcast_to(bias[0:1, :], (128, span)).T

    def tile(b, kv, h, i, j, state):
        there = slice(j * size, (j + 1) * size)
        diagonal = b == 0 and i == j
        later = jnp.where(key_line < query_line, 1.0, 0.0).astype(BF16)
        q = q_ref[pl.ds(pl.multiple_of(h * head_dim, head_dim), head_dim), i * size : (i + 1) * size]
        logits = jnp.dot(kv[there, :head_dim], q, preferred_element_type=F32) * 0.125
        logits = logits + biases_t[b, there, 0:1]
        log_sig = jnp.minimum(logits, 0.0) - jnp.log(1.0 + jnp.exp(-jnp.abs(logits)))
        keep = log_sig - logits
        if diagonal:
            keep = jnp.where(key_line < query_line, keep, 0.0)
        high = keep.astype(BF16)
        low = (keep - high.astype(F32)).astype(BF16)
        after = jnp.dot(later, high, preferred_element_type=F32)
        after = after + jnp.dot(later, low, preferred_element_type=F32)
        weights = jnp.exp(log_sig + after + state[1])
        if diagonal:
            weights = jnp.where(key_line < query_line, weights, 0.0)
        part = jnp.dot(values_t[b, :, there], weights.astype(BF16), preferred_element_type=F32)
        return state[0] + part, state[1] + jnp.sum(keep, axis=0, keepdims=True)

    def attend_own():
        prepare(0, kv_ref, bias_row)

        @pl.loop(0, heads)
        def _(h):
            for i in range(tiles):
                state = (jnp.zeros((head_dim, size), F32), jnp.zeros((1, size), F32))
                for j in range(i, -1, -1):
                    state = tile(0, kv_ref, h, i, j, state)
                att_total[h, i] = state[0]
                att_kept[h, i] = jnp.broadcast_to(state[1], att_kept.shape[2:])

    def attend_next():
        @pl.when(takes_kv)
        def _():
            for which in range(2):
                kv_move(which).wait_recv()
            prepare(1, kv_next, bias_next)

            @pl.loop(0, heads)
            def _(h):
                for i in range(tiles):
                    state = (att_total[h, i], att_kept[h, i, 0:1, :])
                    for j in range(tiles - 1, -1, -1):
                        state = tile(1, kv_next, h, i, j, state)
                    att_total[h, i] = state[0]

    def mixer_pair(k):
        return copy(
            terms.at[3 - 2 * k], mixer_in.at[k], m_send.at[k], m_recv.at[k], z, sibling
        )

    def mixer_move():
        return copy(mixer_sum, mixer_side, m_send.at[2], m_recv.at[2], z, side)

    def project():
        for h in range(heads):
            for i in range(tiles):
                attended_t[h * head_dim : (h + 1) * head_dim, i * size : (i + 1) * size] = (
                    att_total[h, i].astype(BF16)
                )
        loads["out_weight"].wait()
        for r in (3, 1, 2, 0):
            own = pl.ds(pl.multiple_of(places[r] * tokens, tokens), tokens)
            terms[r] = lax.dot_general(
                attended_t[:, own],
                out_weight_v[...],
                (((0,), (0,)), ((), ())),
                preferred_element_type=F32,
            ).astype(BF16)
            if r % 2:
                mixer_pair((3 - r) // 2).start()
        mixer_pair(0).wait_recv()
        mixer_sum[...] = (terms[2].astype(F32) + mixer_in[0].astype(F32)).astype(BF16)

    def shared_expert():
        for name in ("shared_gate", "shared_up", "shared_down"):
            loads[name].wait()
        hidden_gate = jnp.dot(gathered[z], shared_gate_v[...], preferred_element_type=F32)
        hidden_up = jnp.dot(gathered[z], shared_up_v[...], preferred_element_type=F32)
        hidden = (hidden_gate / (1.0 + jnp.exp(-hidden_gate)) * hidden_up).astype(BF16)
        shared[...] = jnp.dot(hidden, shared_down_v[...], preferred_element_type=F32)

    def both(body):
        @pl.loop(0, 2)
        def _(i):
            body(i)

    def arrive(distance, item):
        def body(i):
            zz = z - (2 * i - 1) * distance

            @pl.when(inside(zz))
            def _():
                line(i, zz, item).wait_recv()

                @pl.when(inside(z + 2 * i - 1))
                def _():
                    line(i, zz, item).start()

                if item == 0:
                    meta_wait(0, zz)
                if item == pieces:
                    meta_wait(1, zz)
                    pick_s(zz)
                else:
                    pick(zz, item)

        both(body)

    def result_copy(r, zz, p):
        if p == 0 and r == 3:
            destination, device = rows_in_s.at[zz, band(1)], sibling
        else:
            destination, device = rows_in.at[zz, band(r), columns[p]], places[r]
        return copy(
            chosen.at[zz, band(r), columns[p]],
            destination,
            xr_send.at[r, p, zz],
            xr_recv.at[r, p, zz],
            z,
            device,
        )

    def crossing(p):
        return (1, 3) if p == 0 else (3, 2, 1)

    def feed_forward(zz, send):
        for p in range(pieces):
            for r in crossing(p):
                row_copy(r, zz, p).wait_recv()
        gate = jnp.dot(chosen[zz], gate_v[...], preferred_element_type=F32)
        up = jnp.dot(chosen[zz], up_v[...], preferred_element_type=F32)
        hidden = (gate / (1.0 + jnp.exp(-gate)) * up).astype(BF16)
        for p in range(pieces):
            rows = jnp.dot(hidden, down_v[:, columns[p]], preferred_element_type=F32).astype(BF16)
            chosen[zz, :, columns[p]] = rows
            rows_in[zz, band(0), columns[p]] = rows[band(0)]
            if p == 0:
                rows_in_s[zz, band(0)] = rows[band(2)]
            if send:
                for r in crossing(p):
                    result_copy(r, zz, p).start()

    def feed_forward_at(distance):
        def body(i):
            zz = z - (2 * i - 1) * distance

            @pl.when(inside(zz))
            def _():
                feed_forward(zz, True)

        both(body)

    def send_own_results():
        for p in range(pieces):
            for r in crossing(p):
                result_copy(r, z, p).start()

    def back(i, target, item):
        if item == pieces:
            source, destination = sums_s.at[target], line_in_s.at[i, target]
        else:
            source = sums.at[target, :, columns[item]]
            destination = line_in.at[i, target, :, columns[item]]
        return copy(
            source,
            destination,
            rz_send.at[item, target],
            rz_recv.at[i, item, target],
            z + 2 * i - 1,
            t,
        )

    def total_of(zz, item):
        if item == pieces:
            result_copy(3, zz, 0).wait_recv()
            acc_s[...] = spread(spreader(1, zz, (0, 1)), rows_in_s[zz])
        elif item == 0:
            result_copy(1, zz, 0).wait_recv()
            acc[:, columns[0]] = spread(
                spreader(0, zz, (0, 1)), rows_in[zz, : 2 * capacity, columns[0]]
            )
        else:
            for r in crossing(item):
                result_copy(r, zz, item).wait_recv()
            acc[:, columns[item]] = spread(
                spreader(0, zz, (0, 1, 2, 3)), rows_in[zz, :, columns[item]]
            )

    def take_line(i, zz, item):
        back(i, zz, item).wait_recv()
        if item == pieces:
            acc_s[...] += line_in_s[i, zz].astype(F32)
        else:
            acc[:, columns[item]] += line_in[i, zz, :, columns[item]].astype(F32)

    item_order = (pieces, *range(pieces))

    def stage(s):
        for item in item_order:

            def body(i):
                up = 2 * i - 1
                target = s * i + (count - 1 - s) * (1 - i)

                @pl.when(up * (target - z) > 0)
                def _():
                    total_of(target, item)

                    @pl.when(inside(z - up))
                    def _():
                        take_line(i, target, item)

                    if item == pieces:
                        sums_s[target] = acc_s[...].astype(BF16)
                    else:
                        sums[target, :, columns[item]] = acc[:, columns[item]].astype(BF16)
                    back(i, target, item).start()

            both(body)

    attend_own()
    for distance in range(1, count):
        arrive(distance, 0)
        arrive(distance, 1)
        if distance == 1:
            shared_expert()
        if distance >= 2:
            feed_forward_at(distance - 1)
        if distance == 2:
            project()
        if distance == count - 1:

            @pl.when(jnp.logical_not(is_end))
            def _():
                send_own_results()
                mixer_move().start()

        if distance >= 3:
            stage(distance - 2)
        for item in range(2, items):
            arrive(distance, item)
        if distance == 1:
            for name in ("gate", "up", "down"):
                loads[name].wait()
            feed_forward(z, False)

            @pl.when(is_end)
            def _():
                send_own_results()

            attend_next()

    stage(count - 2)
    feed_forward_at(count - 1)

    @pl.when(is_end)
    def _():
        mixer_move().start()

    stage(count - 1)

    def last_move():
        return copy(sums_s.at[z], from_side, last_send.at[0], last_recv.at[0], z, side)

    for item in item_order:
        total_of(z, item)

        def body(i):
            @pl.when(inside(z - (2 * i - 1)))
            def _():
                take_line(i, z, item)

        both(body)
        if item == pieces:
            sums_s[z] = acc_s[...].astype(BF16)
            last_move().start()
        elif item > 0:
            expert_ref[:, columns[item]] = (
                acc[:, columns[item]] + shared[:, columns[item]]
            ).astype(BF16)
    last_move().wait_recv()
    expert_ref[:, columns[0]] = (
        acc[:, columns[0]] + from_side[...].astype(F32) + shared[:, columns[0]]
    ).astype(BF16)

    mixer_pair(1).wait_recv()
    mixer_move().wait_recv()
    mixer_ref[...] = (
        terms[0].astype(F32) + mixer_in[1].astype(F32) + mixer_side[...].astype(F32)
    ).astype(BF16)

    for step in range(1, count):
        for sx in range(2):
            meta_copy(step, sx).wait_send()
    meta_copy(0, 1).wait_send()
    s_move().wait_send()

    @pl.when(sends_kv)
    def _():
        for which in range(2):
            kv_move(which).wait_send()

    for k in range(2):
        mixer_pair(k).wait_send()
    mixer_move().wait_send()
    last_move().wait_send()

    @pl.loop(0, count)
    def _(zz):
        for p in range(pieces):
            for r in crossing(p):
                row_copy(r, zz, p).wait_send()
                result_copy(r, zz, p).wait_send()
        for item in range(items):
            for i in range(2):
                up = 2 * i - 1

                @pl.when((up * (z - zz) >= 0) & inside(z + up))
                def _():
                    line(i, zz, item).wait_send()

                @pl.when(up * (zz - z) > 0)
                def _():
                    back(i, zz, item).wait_send()


def piece_columns(width):
    unit = width // 8
    edges = (0, 1, 4, 6, 8)
    return [slice(a * unit, b * unit) for a, b in zip(edges, edges[1:])]


def layer(
    queries,
    key_value,
    key_bias,
    out_weight,
    expert_input,
    norm_gain,
    routes,
    route_weights,
    routed_parts,
    shared_parts,
    capacity,
):
    tokens, width = expert_input.shape
    count = lax.axis_size("ep")
    columns = piece_columns(width)
    pieces, cut = len(columns), columns[0].stop
    items = pieces + 1
    span, _, pair_width = key_value.shape
    head_dim = pair_width // 2
    heads = queries.shape[1] // head_dim
    size = min(span, 256)
    hidden = routed_parts[0].shape[1]
    band = 4 * capacity
    dma = pltpu.SemaphoreType.DMA
    vmem = pl.BlockSpec(memory_space=pltpu.VMEM)
    hbm = pl.BlockSpec(memory_space=pl.ANY)
    buffers = [
        ((count, tokens, width), BF16),
        ((count, tokens, cut), BF16),
        ((count, 8, tokens), F32),
        ((2, count, 8, tokens), F32),
        ((count, 3 * capacity, width), BF16),
        ((count, capacity, cut), BF16),
        ((count, band, width), BF16),
        ((count, band, width), BF16),
        ((count, 2 * capacity, cut), BF16),
        ((count, tokens, width), BF16),
        ((count, tokens, cut), BF16),
        ((2, count, tokens, width), BF16),
        ((2, count, tokens, cut), BF16),
        ((tokens, width), F32),
        ((tokens, cut), F32),
        ((tokens, cut), BF16),
        ((tokens, width), F32),
        (out_weight.shape, BF16),
        (shared_parts[0].shape, BF16),
        (shared_parts[1].shape, BF16),
        (shared_parts[2].shape, BF16),
        ((width, hidden), BF16),
        ((width, hidden), BF16),
        ((hidden, width), BF16),
        ((span, pair_width), BF16),
        ((8, span), F32),
        ((8, span), F32),
        ((2, head_dim, span), BF16),
        ((2, span, 128), F32),
        ((heads, span // size, head_dim, size), F32),
        ((heads, span // size, 8, size), F32),
        ((heads * head_dim, span), BF16),
        ((4, tokens, width), BF16),
        ((2, tokens, width), BF16),
        ((tokens, width), BF16),
        ((tokens, width), BF16),
    ]
    semaphores = [
        (7,),
        (2, count),
        (2, count),
        (2,),
        (2,),
        (2, items, count),
        (items, count),
        (1,),
        (1,),
        (4, pieces, count),
        (4, pieces, count),
        (4, pieces, count),
        (4, pieces, count),
        (items, count),
        (2, items, count),
        (1,),
        (1,),
        (3,),
        (3,),
    ]
    return pl.pallas_call(
        lambda *refs: layer_kernel(capacity, *refs),
        out_shape=[jax.ShapeDtypeStruct((tokens, width), BF16)] * 2,
        in_specs=[vmem] * 7 + [hbm] * 7,
        out_specs=[vmem] * 2,
        scratch_shapes=[pltpu.VMEM(*b) for b in buffers] + [dma(s) for s in semaphores],
        compiler_params=pltpu.CompilerParams(
            collective_id=0, has_side_effects=True, vmem_limit_bytes=60 * 2**20
        ),
        name="layer",
        cost_estimate=pl.CostEstimate(flops=10**10, bytes_accessed=2 * 10**7, transcendentals=0),
    )(
        queries.T,
        key_value.reshape(span, pair_width),
        key_bias,
        expert_input,
        norm_gain.reshape(1, width),
        routes.T,
        route_weights.T,
        out_weight,
        *shared_parts,
        *routed_parts,
    )


def expert_rows(arrived, gate_weight, up_weight, down_weight):
    sources, capacity, model_width = arrived.shape
    flat_rows = arrived.reshape(sources * capacity, model_width)
    gate_part = jnp.dot(flat_rows, gate_weight[0], preferred_element_type=jnp.float32)
    up_part = jnp.dot(flat_rows, up_weight[0], preferred_element_type=jnp.float32)
    hidden = (jax.nn.silu(gate_part) * up_part).astype(jnp.bfloat16)
    result = jnp.dot(hidden, down_weight[0], preferred_element_type=jnp.float32).astype(
        jnp.bfloat16
    )
    return result.reshape(sources, capacity, model_width)


def experts_half(
    expert_input,
    norm_gain,
    routes,
    route_weights,
    gate_weight,
    up_weight,
    down_weight,
    shared_gate,
    shared_up,
    shared_down,
):
    tokens, top_count = routes.shape
    model_width = expert_input.shape[1]
    ep_count = lax.axis_size("ep")
    tp_count = lax.axis_size("tp")
    experts = ep_count * tp_count
    capacity = max(2, 3 * tokens * top_count // (2 * experts))
    widened = expert_input.astype(jnp.float32)
    normed = (
        widened * lax.rsqrt(jnp.mean(widened * widened, axis=-1, keepdims=True) + 1e-06) * norm_gain
    ).astype(jnp.bfloat16)
    flat_routes = routes.reshape(-1)
    one_hot = (flat_routes[:, None] == jnp.arange(experts, dtype=jnp.int32)[None, :]).astype(
        jnp.int32
    )
    before = jnp.cumsum(one_hot, axis=0) - one_hot
    slot_index = jnp.sum(before * one_hot, axis=1)
    target = flat_routes * capacity + slot_index
    picker = (jnp.arange(experts * capacity, dtype=jnp.int32)[:, None] == target[None, :]).astype(
        jnp.bfloat16
    )
    picker = jnp.sum(picker.reshape(experts * capacity, tokens, top_count), axis=2)
    outgoing = jnp.dot(picker, normed, preferred_element_type=jnp.float32).astype(jnp.bfloat16)
    outgoing = outgoing.reshape(experts, capacity, model_width)
    came_back = lax.all_to_all(
        expert_rows(
            lax.all_to_all(outgoing, ("ep", "tp"), split_axis=0, concat_axis=0, tiled=True),
            gate_weight,
            up_weight,
            down_weight,
        ),
        ("ep", "tp"),
        split_axis=0,
        concat_axis=0,
        tiled=True,
    )
    back_rows = came_back.reshape(experts * capacity, model_width)
    picked = jnp.take(back_rows, target, axis=0).reshape(tokens, top_count, model_width)
    routed = jnp.sum(picked.astype(jnp.float32) * route_weights[:, :, None], axis=1)
    shared_hidden = (
        jax.nn.silu(jnp.dot(normed, shared_gate, preferred_element_type=jnp.float32))
        * jnp.dot(normed, shared_up, preferred_element_type=jnp.float32)
    ).astype(jnp.bfloat16)
    shared_term = jnp.dot(shared_hidden, shared_down, preferred_element_type=jnp.float32)
    return (routed + shared_term).astype(jnp.bfloat16)


def per_device(
    queries,
    key_value,
    key_bias,
    out_weight,
    expert_input,
    norm_gain,
    routes,
    route_weights,
    gate_weight,
    up_weight,
    down_weight,
    shared_gate,
    shared_up,
    shared_down,
):
    tokens, top_count = routes.shape
    span, key_groups, pair_width = key_value.shape
    width = expert_input.shape[1]
    ep_count, tp_count = lax.axis_size("ep"), lax.axis_size("tp")
    experts = ep_count * tp_count
    capacity = max(2, 3 * tokens * top_count // (2 * experts))
    fits = experts * tokens * width * 2 <= 8 * 2**20 and capacity % 16 == 0 and ep_count >= 3
    whole = tp_count == 4 and span == tp_count * tokens and tokens == 128
    heads_fit = key_groups == 1 and pair_width == 128 and width % 1024 == 0
    if fits and whole and heads_fit and furthest_place(ep_count) <= 1:
        return tuple(
            layer(
                queries,
                key_value,
                key_bias,
                out_weight,
                expert_input,
                norm_gain,
                routes,
                route_weights,
                (gate_weight[0], up_weight[0], down_weight[0]),
                (shared_gate, shared_up, shared_down),
                capacity,
            )
        )
    terms = project(attend(queries, key_value, key_bias), out_weight)
    mixer_output = lax.psum_scatter(terms, "tp", scatter_dimension=0, tiled=True)
    expert_output = experts_half(
        expert_input,
        norm_gain,
        routes,
        route_weights,
        gate_weight,
        up_weight,
        down_weight,
        shared_gate,
        shared_up,
        shared_down,
    )
    return (mixer_output, expert_output)


def solution(mesh):
    placed = (
        P(("grp", "ep"), "tp"),
        P(("grp", "ep"), "tp", None),
        P("tp", ("grp", "ep")),
        P("tp", None),
        P(("grp", "ep", "tp"), None),
        P(),
        P(("grp", "ep", "tp"), None),
        P(("grp", "ep", "tp"), None),
        P(("ep", "tp"), None, None),
        P(("ep", "tp"), None, None),
        P(("ep", "tp"), None, None),
        P(),
        P(),
        P(),
    )
    return jax.shard_map(
        per_device,
        mesh=mesh,
        in_specs=placed,
        out_specs=(P(("grp", "ep", "tp"), None), P(("grp", "ep", "tp"), None)),
        check_vma=False,
    )
```

```python
import jax
import jax.numpy as jnp
from jax import lax
from jax.experimental import pallas as pl
from jax.experimental.pallas import tpu as pltpu
from jax.sharding import PartitionSpec as P

MESH = pl.DeviceIdType.MESH
F32 = jnp.float32
BF16 = jnp.bfloat16


def passed_along(block, axis, distance):
    devices = range(lax.axis_size(axis))
    route = [(i - distance, i) for i in devices if i - distance in devices]
    return lax.ppermute(block, axis, route)


def furthest_place(axis_size):
    chain_length = axis_size // max(1, axis_size // 4)
    return max(min((p + 2) % chain_length, p) for p in range(axis_size))


def attention_tile(q, k, v, bias, upper, kept, masked):
    z = lax.dot_general(q, k, (((1,), (1,)), ((), ())), preferred_element_type=F32) * 0.125 + bias
    tail = jnp.log(1.0 + jnp.exp(-jnp.abs(z)))
    log_sig = jnp.minimum(z, 0.0) - tail
    keep = -(jnp.maximum(z, 0.0) + tail)
    if masked:
        rows = lax.broadcasted_iota(jnp.int32, z.shape, 0)
        columns = lax.broadcasted_iota(jnp.int32, z.shape, 1)
        allowed = columns < rows
        keep = jnp.where(allowed, keep, 0.0)
    high = keep.astype(BF16)
    low = (keep - high.astype(F32)).astype(BF16)
    after = jnp.dot(high, upper, preferred_element_type=F32)
    after = after + jnp.dot(low, upper, preferred_element_type=F32)
    weight = jnp.exp(log_sig + after + kept)
    if masked:
        weight = jnp.where(allowed, weight, 0.0)
    part = jnp.dot(weight.astype(BF16), v, preferred_element_type=F32)
    return part, kept + jnp.sum(keep, axis=1, keepdims=True)


def attention_kernel(place_ref, q_ref, kv_ref, bias_ref, out_ref, total, kept):
    span, head_dim = q_ref.shape[1:]
    spans = kv_ref.shape[0]
    size = min(span, 256)
    tiles = span // size
    rows = lax.broadcasted_iota(jnp.int32, (size, size), 0)
    columns = lax.broadcasted_iota(jnp.int32, (size, size), 1)
    upper = jnp.where(rows > columns, 1.0, 0.0).astype(BF16)

    def tile(distance, i, j, masked, state):
        there = pl.ds(j * size, size)
        part, after = attention_tile(
            q_ref[0, i * size : (i + 1) * size, :],
            kv_ref[distance, 0, there, :head_dim],
            kv_ref[distance, 0, there, head_dim:],
            bias_ref[distance, 0, :, there].astype(F32),
            upper,
            state[1],
            masked,
        )
        return state[0] + part, after

    for i in range(tiles):
        state = (jnp.zeros((size, head_dim), F32), jnp.zeros((size, 1), F32))
        for j in range(i, -1, -1):
            state = tile(0, i, j, j == i, state)
        total[i] = state[0]
        kept[i] = jnp.broadcast_to(state[1], kept.shape[1:])
    for distance in range(1, spans):

        @pl.when(distance <= place_ref[0])
        def _():
            for i in range(tiles):
                state = (total[i], kept[i, :, :1])
                for j in range(tiles - 1, -1, -1):
                    state = tile(distance, i, j, False, state)
                total[i] = state[0]
                kept[i] = jnp.broadcast_to(state[1], kept.shape[1:])

    for i in range(tiles):
        out_ref[0, i * size : (i + 1) * size, :] = total[i].astype(out_ref.dtype)


def attend(queries, key_value, key_bias):
    span, key_groups, pair_width = key_value.shape
    head_dim = pair_width // 2
    heads = queries.shape[1] // head_dim
    per_group = heads // key_groups
    axis_size = lax.axis_size("ep")
    chain_length = axis_size // max(1, axis_size // 4)
    place = lax.axis_index("ep")
    chain_place = jnp.minimum((place + 2) % chain_length, place)
    furthest = furthest_place(axis_size)
    packed = jnp.concatenate([key_value.reshape(-1, pair_width), key_bias.reshape(-1, pair_width)])
    visiting = [packed]
    for _ in range(furthest):
        visiting.append(passed_along(visiting[-1], "ep", 1))
    visiting = jnp.stack(visiting)
    keys = visiting[:, : span * key_groups].reshape(-1, span, key_groups, pair_width)
    keys = keys.transpose(0, 2, 1, 3)
    biases = visiting[:, span * key_groups :].reshape(-1, key_groups, 1, span)
    size = min(span, 256)
    attended = pl.pallas_call(
        attention_kernel,
        grid=(heads,),
        out_shape=jax.ShapeDtypeStruct((heads, span, head_dim), BF16),
        in_specs=[
            pl.BlockSpec(memory_space=pltpu.SMEM),
            pl.BlockSpec((1, span, head_dim), lambda h: (h, 0, 0)),
            pl.BlockSpec((furthest + 1, 1, span, pair_width), lambda h: (0, h // per_group, 0, 0)),
            pl.BlockSpec((furthest + 1, 1, 1, span), lambda h: (0, h // per_group, 0, 0)),
        ],
        out_specs=pl.BlockSpec((1, span, head_dim), lambda h: (h, 0, 0)),
        scratch_shapes=[
            pltpu.VMEM((span // size, size, head_dim), F32),
            pltpu.VMEM((span // size, size, 128), F32),
        ],
        name="attention",
        cost_estimate=pl.CostEstimate(flops=4 * 10**9, bytes_accessed=10**6, transcendentals=0),
    )(
        chain_place.reshape(1),
        queries.reshape(span, heads, head_dim).transpose(1, 0, 2),
        keys,
        biases,
    )
    return attended.transpose(1, 0, 2).reshape(span, heads * head_dim)


def project(attended, out_weight):
    return jnp.dot(attended, out_weight, preferred_element_type=F32).astype(BF16)


def layer_kernel(
    capacity,
    q_ref,
    kv_ref,
    bias_ref,
    x_ref,
    gain_ref,
    routes_ref,
    route_weights_ref,
    out_weight_hbm,
    shared_gate_hbm,
    shared_up_hbm,
    shared_down_hbm,
    gate_hbm,
    up_hbm,
    down_hbm,
    mixer_ref,
    expert_ref,
    gathered,
    gathered_s,
    meta_out,
    meta,
    staged,
    staged_s,
    chosen,
    rows_in,
    rows_in_s,
    sums,
    sums_s,
    line_in,
    line_in_s,
    acc,
    acc_s,
    from_side,
    shared,
    out_weight_v,
    shared_gate_v,
    shared_up_v,
    shared_down_v,
    gate_v,
    up_v,
    down_v,
    kv_next,
    bias_row,
    bias_next,
    values_t,
    biases_t,
    att_total,
    att_kept,
    attended_t,
    terms,
    mixer_in,
    mixer_sum,
    mixer_side,
    load_sem,
    meta_send,
    meta_recv,
    kv_send,
    kv_recv,
    zs_send,
    zs_recv,
    s_send,
    s_recv,
    xa_send,
    xa_recv,
    xr_send,
    xr_recv,
    rz_send,
    rz_recv,
    last_send,
    last_recv,
    m_send,
    m_recv,
):
    count = lax.axis_size("ep")
    tokens, width = x_ref.shape
    columns = piece_columns(width)
    pieces = len(columns)
    cut = columns[0].stop
    items = pieces + 1
    z = lax.axis_index("ep")
    t = lax.axis_index("tp")
    x, c = t // 2, t % 2
    ox, oc = 1 - x, 1 - c
    places = (t, x * 2 + oc, ox * 2 + c, ox * 2 + oc)
    sibling, side = places[1], places[2]
    is_end = (z == 0) | (z == count - 1)

    def inside(zz):
        return (zz >= 0) & (zz < count)

    def copy(src, dst, send, recv, ep, tp):
        return pltpu.make_async_remote_copy(
            src_ref=src,
            dst_ref=dst,
            send_sem=send,
            recv_sem=recv,
            device_id={"ep": ep, "tp": tp},
            device_id_type=MESH,
        )

    def band(r):
        return slice(r * capacity, (r + 1) * capacity)

    loads = {
        name: pltpu.make_async_copy(a, b, load_sem.at[i])
        for i, (name, a, b) in enumerate(
            (
                ("shared_gate", shared_gate_hbm, shared_gate_v),
                ("shared_up", shared_up_hbm, shared_up_v),
                ("shared_down", shared_down_hbm, shared_down_v),
                ("gate", gate_hbm, gate_v),
                ("up", up_hbm, up_v),
                ("down", down_hbm, down_v),
                ("out_weight", out_weight_hbm, out_weight_v),
            )
        )
    }

    barrier = pltpu.get_barrier_semaphore()

    def greet(ep, tp):
        pl.semaphore_signal(barrier, 1, device_id={"ep": ep, "tp": tp}, device_id_type=MESH)

    for step in range(1, count):
        for sx in (0, 2):
            greet((z + step) % count, places[sx])
    for r in (1, 2, 3):
        greet(z, places[r])

    @pl.loop(0, tokens // 16)
    def _(block):
        rows = pl.ds(pl.multiple_of(block * 16, 16), 16)
        wide = x_ref[rows, :].astype(F32)
        mean = jnp.mean(wide * wide, axis=-1, keepdims=True)
        gathered[z, rows, :] = (wide * lax.rsqrt(mean + 1e-06) * gain_ref[...]).astype(BF16)

    lines = lax.broadcasted_iota(jnp.int32, (count * 8, tokens), 0)
    expert = (lines // 8) * 4 + lines % 4
    named = jnp.zeros((count * 8, tokens), F32)
    weight = jnp.zeros((count * 8, tokens), F32)
    for k in range(routes_ref.shape[0]):
        hit = routes_ref[k : k + 1, :] == expert
        named = named + jnp.where(hit, 1.0, 0.0)
        weight = weight + jnp.where(hit, route_weights_ref[k : k + 1, :], 0.0)
    before = lax.broadcasted_iota(jnp.int32, (tokens, tokens), 0) < lax.broadcasted_iota(
        jnp.int32, (tokens, tokens), 1
    )
    slot = jnp.dot(
        named.astype(BF16), jnp.where(before, 1.0, 0.0).astype(BF16), preferred_element_type=F32
    )
    slot = jnp.where(named > 0.5, slot, -1.0)
    meta_out[...] = jnp.where(lines % 8 < 4, slot, weight).reshape(meta_out.shape)
    meta[0, z] = meta_out[z]
    bias_row[...] = jnp.broadcast_to(bias_ref[...].astype(F32), bias_row.shape)

    pl.semaphore_wait(barrier, 2 * (count - 1) + 3)

    def meta_copy(step, sx):
        other = (z + step) % count
        return copy(
            meta_out.at[other],
            meta.at[sx, z],
            meta_send.at[sx, step],
            meta_recv.at[sx, z],
            other,
            places[2 * sx],
        )

    def meta_wait(sx, zz):
        copy(
            meta_out.at[zz], meta.at[sx, zz], meta_send.at[sx, 0], meta_recv.at[sx, zz], z, side
        ).wait_recv()

    def s_move():
        return copy(
            gathered.at[z, :, columns[0]], gathered_s.at[z], s_send.at[0], s_recv.at[0], z, side
        )

    def line(i, zz, item):
        small = 1 if item == pieces else 0
        block = gathered_s.at[zz] if small else gathered.at[zz, :, columns[item]]
        return copy(
            block, block, zs_send.at[i, small, zz], zs_recv.at[item, zz], z + 2 * i - 1, t
        )

    def kv_move(which):
        pair = ((kv_ref, kv_next), (bias_row, bias_next))[which]
        return copy(*pair, kv_send.at[which], kv_recv.at[which], z + 1, t)

    chain = count // max(1, count // 4)

    def chain_place(zz):
        return jnp.minimum((zz + 2) % chain, zz)

    sends_kv = (z + 1 < count) & (chain_place(z + 1) >= 1)
    takes_kv = chain_place(z) >= 1

    for step in range(1, count):
        for sx in range(2):
            meta_copy(step, sx).start()
    meta_copy(0, 1).start()
    s_move().start()
    for item in range(pieces):
        for i in range(2):

            @pl.when(inside(z + 2 * i - 1))
            def _():
                line(i, z, item).start()

    slots = lax.broadcasted_iota(jnp.int32, (capacity, tokens), 0).astype(F32)

    def one_hot(sx, zz, rels):
        return jnp.concatenate(
            [jnp.where(meta[sx, zz, pl.ds(places[r], 1), :] == slots, 1.0, 0.0) for r in rels],
            axis=0,
        ).astype(BF16)

    def spreader(sx, zz, rels):
        weights = jnp.concatenate(
            [
                jnp.where(
                    meta[sx, zz, pl.ds(places[r], 1), :] == slots,
                    meta[sx, zz, pl.ds(4 + places[r], 1), :],
                    0.0,
                )
                for r in rels
            ],
            axis=0,
        )
        high = weights.astype(BF16)
        return high, (weights - high.astype(F32)).astype(BF16)

    def spread(pair, rows):
        return sum(
            lax.dot_general(half, rows, (((0,), (0,)), ((), ())), preferred_element_type=F32)
            for half in pair
        )

    def row_copy(r, zz, p):
        if p == 0 and r == 3:
            return copy(
                staged_s.at[zz],
                chosen.at[zz, band(3), columns[0]],
                xa_send.at[r],
                xa_recv.at[r, zz],
                z,
                sibling,
            )
        return copy(
            staged.at[zz, band(r - 1), columns[p]],
            chosen.at[zz, band(r), columns[p]],
            xa_send.at[r],
            xa_recv.at[r, zz],
            z,
            places[r],
        )

    def pick(zz, p):
        rels = (0, 1) if p == 0 else (0, 1, 2, 3)
        picked = jnp.dot(
            one_hot(0, zz, rels), gathered[zz, :, columns[p]], preferred_element_type=F32
        ).astype(BF16)
        staged[zz, : (len(rels) - 1) * capacity, columns[p]] = picked[capacity:]
        chosen[zz, band(0), columns[p]] = picked[:capacity]
        for r in rels[:0:-1]:
            row_copy(r, zz, p).start()

    def pick_s(zz):
        picked = jnp.dot(
            one_hot(1, zz, (0, 1)), gathered_s[zz], preferred_element_type=F32
        ).astype(BF16)
        staged_s[zz] = picked[capacity:]
        chosen[zz, band(2), columns[0]] = picked[:capacity]
        row_copy(3, zz, 0).start()

    for p in (*range(1, pieces), 0):
        pick(z, p)
    s_move().wait_recv()
    for i in range(2):

        @pl.when(inside(z + 2 * i - 1))
        def _():
            line(i, z, pieces).start()

    @pl.when(sends_kv)
    def _():
        kv_move(1).start()
        kv_move(0).start()

    for load in loads.values():
        load.start()
    meta_wait(1, z)
    pick_s(z)

    span = kv_ref.shape[0]
    head_dim = kv_ref.shape[1] // 2
    heads = q_ref.shape[0] // head_dim
    size = min(span, 256)
    tiles = span // size
    key_line = lax.broadcasted_iota(jnp.int32, (size, size), 0)
    query_line = lax.broadcasted_iota(jnp.int32, (size, size), 1)

    def prepare(b, kv, bias):
        values_t[b] = kv[...].astype(F32).T[head_dim:, :].astype(BF16)
        biases_t[b] = jnp.broadcast_to(bias[0:1, :], (128, span)).T

    def tile(b, kv, h, i, j, state):
        there = slice(j * size, (j + 1) * size)
        diagonal = b == 0 and i == j
        later = jnp.where(key_line < query_line, 1.0, 0.0).astype(BF16)
        q = q_ref[pl.ds(pl.multiple_of(h * head_dim, head_dim), head_dim), i * size : (i + 1) * size]
        logits = jnp.dot(kv[there, :head_dim], q, preferred_element_type=F32) * 0.125
        logits = logits + biases_t[b, there, 0:1]
        log_sig = jnp.minimum(logits, 0.0) - jnp.log(1.0 + jnp.exp(-jnp.abs(logits)))
        keep = log_sig - logits
        if diagonal:
            keep = jnp.where(key_line < query_line, keep, 0.0)
        high = keep.astype(BF16)
        low = (keep - high.astype(F32)).astype(BF16)
        after = jnp.dot(later, high, preferred_element_type=F32)
        after = after + jnp.dot(later, low, preferred_element_type=F32)
        weights = jnp.exp(log_sig + after + state[1])
        if diagonal:
            weights = jnp.where(key_line < query_line, weights, 0.0)
        part = jnp.dot(values_t[b, :, there], weights.astype(BF16), preferred_element_type=F32)
        return state[0] + part, state[1] + jnp.sum(keep, axis=0, keepdims=True)

    def attend_own():
        prepare(0, kv_ref, bias_row)

        @pl.loop(0, heads)
        def _(h):
            for i in range(tiles):
                state = (jnp.zeros((head_dim, size), F32), jnp.zeros((1, size), F32))
                for j in range(i, -1, -1):
                    state = tile(0, kv_ref, h, i, j, state)
                att_total[h, i] = state[0]
                att_kept[h, i] = jnp.broadcast_to(state[1], att_kept.shape[2:])

    def attend_next(first, low, high):
        @pl.when(takes_kv)
        def _():
            if first:
                for which in range(2):
                    kv_move(which).wait_recv()
                prepare(1, kv_next, bias_next)

            @pl.loop(low, high)
            def _(h):
                for i in range(tiles):
                    state = (att_total[h, i], att_kept[h, i, 0:1, :])
                    for j in range(tiles - 1, -1, -1):
                        state = tile(1, kv_next, h, i, j, state)
                    att_total[h, i] = state[0]

    def mixer_pair(k):
        return copy(
            terms.at[3 - 2 * k], mixer_in.at[k], m_send.at[k], m_recv.at[k], z, sibling
        )

    def mixer_move():
        return copy(mixer_sum, mixer_side, m_send.at[2], m_recv.at[2], z, side)

    def project():
        for h in range(heads):
            for i in range(tiles):
                attended_t[h * head_dim : (h + 1) * head_dim, i * size : (i + 1) * size] = (
                    att_total[h, i].astype(BF16)
                )
        loads["out_weight"].wait()
        for r in (3, 1, 2, 0):
            own = pl.ds(pl.multiple_of(places[r] * tokens, tokens), tokens)
            terms[r] = lax.dot_general(
                attended_t[:, own],
                out_weight_v[...],
                (((0,), (0,)), ((), ())),
                preferred_element_type=F32,
            ).astype(BF16)
            if r % 2:
                mixer_pair((3 - r) // 2).start()
        mixer_pair(0).wait_recv()
        mixer_sum[...] = (terms[2].astype(F32) + mixer_in[0].astype(F32)).astype(BF16)

    def shared_expert():
        for name in ("shared_gate", "shared_up", "shared_down"):
            loads[name].wait()
        hidden_gate = jnp.dot(gathered[z], shared_gate_v[...], preferred_element_type=F32)
        hidden_up = jnp.dot(gathered[z], shared_up_v[...], preferred_element_type=F32)
        hidden = (hidden_gate / (1.0 + jnp.exp(-hidden_gate)) * hidden_up).astype(BF16)
        shared[...] = jnp.dot(hidden, shared_down_v[...], preferred_element_type=F32)

    def both(body):
        @pl.loop(0, 2)
        def _(i):
            body(i)

    def arrive(distance, item):
        def body(i):
            zz = z - (2 * i - 1) * distance

            @pl.when(inside(zz))
            def _():
                line(i, zz, item).wait_recv()

                @pl.when(inside(z + 2 * i - 1))
                def _():
                    line(i, zz, item).start()

                if item == 0:
                    meta_wait(0, zz)
                if item == pieces:
                    meta_wait(1, zz)
                    pick_s(zz)
                else:
                    pick(zz, item)

        both(body)

    def result_copy(r, zz, p):
        if p == 0 and r == 3:
            destination, device = rows_in_s.at[zz, band(1)], sibling
        else:
            destination, device = rows_in.at[zz, band(r), columns[p]], places[r]
        return copy(
            chosen.at[zz, band(r), columns[p]],
            destination,
            xr_send.at[r],
            xr_recv.at[r, p, zz],
            z,
            device,
        )

    def reach(r):
        return slice(cut if r == 2 else 0, width)

    def crossing(p):
        return (1, 3) if p == 0 else (3, 2, 1)

    def send_results(zz):
        for p in range(pieces):
            for r in crossing(p):
                result_copy(r, zz, p).start()

    def feed_forward(zz, send):
        for r in (1, 2, 3):
            arrived = chosen.at[zz, band(r), reach(r)]
            copy(arrived, arrived, xa_send.at[r], xa_recv.at[r, zz], z, sibling).wait_recv()
        gate = jnp.dot(chosen[zz], gate_v[...], preferred_element_type=F32)
        up = jnp.dot(chosen[zz], up_v[...], preferred_element_type=F32)
        hidden = (gate / (1.0 + jnp.exp(-gate)) * up).astype(BF16)
        for p in range(pieces):
            rows = jnp.dot(hidden, down_v[:, columns[p]], preferred_element_type=F32).astype(BF16)
            chosen[zz, :, columns[p]] = rows
            rows_in[zz, band(0), columns[p]] = rows[band(0)]
            if p == 0:
                rows_in_s[zz, band(0)] = rows[band(2)]


            if send:
                for r in crossing(p):
                    result_copy(r, zz, p).start()

    def feed_forward_at(distance):
        def body(i):
            zz = z - (2 * i - 1) * distance

            @pl.when(inside(zz))
            def _():
                feed_forward(zz, True)

        both(body)

    def back(i, target, item):
        if item == pieces:
            source, destination = sums_s.at[target], line_in_s.at[i, target]
        else:
            source = sums.at[target, :, columns[item]]
            destination = line_in.at[i, target, :, columns[item]]
        return copy(
            source,
            destination,
            rz_send.at[1 if item == pieces else 0, target],
            rz_recv.at[i, item, target],
            z + 2 * i - 1,
            t,
        )

    def total_of(zz, item):
        if item == pieces:
            result_copy(3, zz, 0).wait_recv()
            acc_s[...] = spread(spreader(1, zz, (0, 1)), rows_in_s[zz])
        elif item == 0:
            result_copy(1, zz, 0).wait_recv()
            acc[:, columns[0]] = spread(
                spreader(0, zz, (0, 1)), rows_in[zz, : 2 * capacity, columns[0]]
            )
        else:
            for r in crossing(item):
                result_copy(r, zz, item).wait_recv()
            acc[:, columns[item]] = spread(
                spreader(0, zz, (0, 1, 2, 3)), rows_in[zz, :, columns[item]]
            )

    def take_line(i, zz, item):
        back(i, zz, item).wait_recv()
        if item == pieces:
            acc_s[...] += line_in_s[i, zz].astype(F32)
        else:
            acc[:, columns[item]] += line_in[i, zz, :, columns[item]].astype(F32)

    item_order = (pieces, *range(pieces))

    near = jnp.where(2 * z < count, 1, 0)

    def stage_item(s, i, item):
        up = 2 * i - 1
        target = s * i + (count - 1 - s) * (1 - i)

        @pl.when(up * (target - z) > 0)
        def _():
            total_of(target, item)

            @pl.when(inside(z - up))
            def _():
                take_line(i, target, item)

            if item == pieces:
                sums_s[target] = acc_s[...].astype(BF16)
            else:
                sums[target, :, columns[item]] = acc[:, columns[item]].astype(BF16)
            back(i, target, item).start()

    def stage(s):
        for k in range(items + 2):
            if k < items:
                stage_item(s, near, item_order[k])
            if k >= 2:
                stage_item(s, 1 - near, item_order[k - 2])

    attend_own()
    arrive(1, 0)
    arrive(1, 1)
    shared_expert()
    for item in range(2, items):
        arrive(1, item)
    for name in ("gate", "up", "down"):
        loads[name].wait()
    feed_forward(z, False)
    for distance in range(2, count):
        last = distance == count - 1
        if not last:
            pl.when(is_end)(lambda: feed_forward_at(distance - 1))
        for item in range(items):
            if last and item == 3:
                feed_forward_at(distance - 1)

                @pl.when(jnp.logical_not(is_end))
                def _():
                    send_results(z)

            if distance == 2 and item in (2, 4):
                attend_next(item == 2, 0 if item == 2 else heads // 2, heads // 2 if item == 2 else heads - 1)
            if last and item == 2:
                attend_next(False, heads - 1, heads)
            arrive(distance, item)
        if not last:
            pl.when(jnp.logical_not(is_end))(lambda: feed_forward_at(distance - 1))
            stage(distance - 1)

    @pl.when(jnp.logical_not(is_end))
    def _():
        project()
        mixer_move().start()

    stage(count - 2)
    feed_forward_at(count - 1)

    @pl.when(is_end)
    def _():
        send_results(z)
        project()
        mixer_move().start()

    stage(count - 1)

    def last_move():
        return copy(sums_s.at[z], from_side, last_send.at[0], last_recv.at[0], z, side)

    for item in item_order:
        total_of(z, item)

        def body(i):
            @pl.when(inside(z - (2 * i - 1)))
            def _():
                take_line(i, z, item)

        both(body)
        if item == pieces:
            sums_s[z] = acc_s[...].astype(BF16)
            last_move().start()
        elif item > 0:
            expert_ref[:, columns[item]] = (
                acc[:, columns[item]] + shared[:, columns[item]]
            ).astype(BF16)
    last_move().wait_recv()
    expert_ref[:, columns[0]] = (
        acc[:, columns[0]] + from_side[...].astype(F32) + shared[:, columns[0]]
    ).astype(BF16)

    mixer_pair(1).wait_recv()
    mixer_move().wait_recv()
    mixer_ref[...] = (
        terms[0].astype(F32) + mixer_in[1].astype(F32) + mixer_side[...].astype(F32)
    ).astype(BF16)

    for step in range(1, count):
        for sx in range(2):
            meta_copy(step, sx).wait_send()
    meta_copy(0, 1).wait_send()
    s_move().wait_send()

    @pl.when(sends_kv)
    def _():
        for which in range(2):
            kv_move(which).wait_send()

    for k in range(2):
        mixer_pair(k).wait_send()
    mixer_move().wait_send()
    last_move().wait_send()

    for r in (1, 2, 3):
        for sent, send in (
            (staged.at[:, band(r - 1), reach(r)], xa_send),
            (chosen.at[:, band(r), reach(r)], xr_send),
        ):
            copy(sent, sent, send.at[r], xa_recv.at[r, 0], z, sibling).wait_send()

    @pl.loop(0, count)
    def _(zz):
        for small in range(2):
            gather, reduce = ((gathered, sums), (gathered_s, sums_s))[small]
            for i in range(2):
                up = 2 * i - 1

                @pl.when((up * (z - zz) >= 0) & inside(z + up))
                def _():
                    sent = gather.at[zz]
                    copy(
                        sent, sent, zs_send.at[i, small, zz], zs_recv.at[0, zz], z, sibling
                    ).wait_send()

            @pl.when(zz != z)
            def _():
                sent = reduce.at[zz]
                copy(sent, sent, rz_send.at[small, zz], zs_recv.at[0, zz], z, sibling).wait_send()


def piece_columns(width):
    unit = width // 16
    edges = (0, 2, 5, 8, 10, 12, 14, 16)
    return [slice(a * unit, b * unit) for a, b in zip(edges, edges[1:])]


def layer(
    queries,
    key_value,
    key_bias,
    out_weight,
    expert_input,
    norm_gain,
    routes,
    route_weights,
    routed_parts,
    shared_parts,
    capacity,
):
    tokens, width = expert_input.shape
    count = lax.axis_size("ep")
    columns = piece_columns(width)
    pieces, cut = len(columns), columns[0].stop
    items = pieces + 1
    span, _, pair_width = key_value.shape
    head_dim = pair_width // 2
    heads = queries.shape[1] // head_dim
    size = min(span, 256)
    hidden = routed_parts[0].shape[1]
    band = 4 * capacity
    dma = pltpu.SemaphoreType.DMA
    vmem = pl.BlockSpec(memory_space=pltpu.VMEM)
    hbm = pl.BlockSpec(memory_space=pl.ANY)
    buffers = [
        ((count, tokens, width), BF16),
        ((count, tokens, cut), BF16),
        ((count, 8, tokens), F32),
        ((2, count, 8, tokens), F32),
        ((count, 3 * capacity, width), BF16),
        ((count, capacity, cut), BF16),
        ((count, band, width), BF16),
        ((count, band, width), BF16),
        ((count, 2 * capacity, cut), BF16),
        ((count, tokens, width), BF16),
        ((count, tokens, cut), BF16),
        ((2, count, tokens, width), BF16),
        ((2, count, tokens, cut), BF16),
        ((tokens, width), F32),
        ((tokens, cut), F32),
        ((tokens, cut), BF16),
        ((tokens, width), F32),
        (out_weight.shape, BF16),
        (shared_parts[0].shape, BF16),
        (shared_parts[1].shape, BF16),
        (shared_parts[2].shape, BF16),
        ((width, hidden), BF16),
        ((width, hidden), BF16),
        ((hidden, width), BF16),
        ((span, pair_width), BF16),
        ((8, span), F32),
        ((8, span), F32),
        ((2, head_dim, span), BF16),
        ((2, span, 128), F32),
        ((heads, span // size, head_dim, size), F32),
        ((heads, span // size, 8, size), F32),
        ((heads * head_dim, span), BF16),
        ((4, tokens, width), BF16),
        ((2, tokens, width), BF16),
        ((tokens, width), BF16),
        ((tokens, width), BF16),
    ]
    semaphores = [
        (7,),
        (2, count),
        (2, count),
        (2,),
        (2,),
        (2, 2, count),
        (items, count),
        (1,),
        (1,),
        (4,),
        (4, count),
        (4,),
        (4, pieces, count),
        (2, count),
        (2, items, count),
        (1,),
        (1,),
        (3,),
        (3,),
    ]
    return pl.pallas_call(
        lambda *refs: layer_kernel(capacity, *refs),
        out_shape=[pltpu.VMEM((tokens, width), BF16)] * 2,
        in_specs=[vmem] * 7 + [hbm] * 7,
        out_specs=[vmem] * 2,
        scratch_shapes=[pltpu.VMEM(*b) for b in buffers] + [dma(s) for s in semaphores],
        compiler_params=pltpu.CompilerParams(
            collective_id=0, has_side_effects=True, vmem_limit_bytes=60 * 2**20
        ),
        name="layer",
        cost_estimate=pl.CostEstimate(flops=10**10, bytes_accessed=2 * 10**7, transcendentals=0),
    )(
        queries.T,
        key_value.reshape(span, pair_width),
        key_bias,
        expert_input,
        norm_gain.reshape(1, width),
        routes.T,
        route_weights.T,
        out_weight,
        *shared_parts,
        *routed_parts,
    )


def expert_rows(arrived, gate_weight, up_weight, down_weight):
    sources, capacity, model_width = arrived.shape
    flat_rows = arrived.reshape(sources * capacity, model_width)
    gate_part = jnp.dot(flat_rows, gate_weight[0], preferred_element_type=jnp.float32)
    up_part = jnp.dot(flat_rows, up_weight[0], preferred_element_type=jnp.float32)
    hidden = (jax.nn.silu(gate_part) * up_part).astype(jnp.bfloat16)
    result = jnp.dot(hidden, down_weight[0], preferred_element_type=jnp.float32).astype(
        jnp.bfloat16
    )
    return result.reshape(sources, capacity, model_width)


def experts_half(
    expert_input,
    norm_gain,
    routes,
    route_weights,
    gate_weight,
    up_weight,
    down_weight,
    shared_gate,
    shared_up,
    shared_down,
):
    tokens, top_count = routes.shape
    model_width = expert_input.shape[1]
    ep_count = lax.axis_size("ep")
    tp_count = lax.axis_size("tp")
    experts = ep_count * tp_count
    capacity = max(2, 3 * tokens * top_count // (2 * experts))
    widened = expert_input.astype(jnp.float32)
    normed = (
        widened * lax.rsqrt(jnp.mean(widened * widened, axis=-1, keepdims=True) + 1e-06) * norm_gain
    ).astype(jnp.bfloat16)
    flat_routes = routes.reshape(-1)
    one_hot = (flat_routes[:, None] == jnp.arange(experts, dtype=jnp.int32)[None, :]).astype(
        jnp.int32
    )
    before = jnp.cumsum(one_hot, axis=0) - one_hot
    slot_index = jnp.sum(before * one_hot, axis=1)
    target = flat_routes * capacity + slot_index
    picker = (jnp.arange(experts * capacity, dtype=jnp.int32)[:, None] == target[None, :]).astype(
        jnp.bfloat16
    )
    picker = jnp.sum(picker.reshape(experts * capacity, tokens, top_count), axis=2)
    outgoing = jnp.dot(picker, normed, preferred_element_type=jnp.float32).astype(jnp.bfloat16)
    outgoing = outgoing.reshape(experts, capacity, model_width)
    came_back = lax.all_to_all(
        expert_rows(
            lax.all_to_all(outgoing, ("ep", "tp"), split_axis=0, concat_axis=0, tiled=True),
            gate_weight,
            up_weight,
            down_weight,
        ),
        ("ep", "tp"),
        split_axis=0,
        concat_axis=0,
        tiled=True,
    )
    back_rows = came_back.reshape(experts * capacity, model_width)
    picked = jnp.take(back_rows, target, axis=0).reshape(tokens, top_count, model_width)
    routed = jnp.sum(picked.astype(jnp.float32) * route_weights[:, :, None], axis=1)
    shared_hidden = (
        jax.nn.silu(jnp.dot(normed, shared_gate, preferred_element_type=jnp.float32))
        * jnp.dot(normed, shared_up, preferred_element_type=jnp.float32)
    ).astype(jnp.bfloat16)
    shared_term = jnp.dot(shared_hidden, shared_down, preferred_element_type=jnp.float32)
    return (routed + shared_term).astype(jnp.bfloat16)


def per_device(
    queries,
    key_value,
    key_bias,
    out_weight,
    expert_input,
    norm_gain,
    routes,
    route_weights,
    gate_weight,
    up_weight,
    down_weight,
    shared_gate,
    shared_up,
    shared_down,
):
    tokens, top_count = routes.shape
    span, key_groups, pair_width = key_value.shape
    width = expert_input.shape[1]
    ep_count, tp_count = lax.axis_size("ep"), lax.axis_size("tp")
    experts = ep_count * tp_count
    capacity = max(2, 3 * tokens * top_count // (2 * experts))
    fits = experts * tokens * width * 2 <= 8 * 2**20 and capacity % 16 == 0 and ep_count >= 3
    whole = tp_count == 4 and span == tp_count * tokens and tokens == 128
    heads_fit = key_groups == 1 and pair_width == 128 and width % 1024 == 0
    if fits and whole and heads_fit and furthest_place(ep_count) <= 1:
        return tuple(
            layer(
                queries,
                key_value,
                key_bias,
                out_weight,
                expert_input,
                norm_gain,
                routes,
                route_weights,
                (gate_weight[0], up_weight[0], down_weight[0]),
                (shared_gate, shared_up, shared_down),
                capacity,
            )
        )
    terms = project(attend(queries, key_value, key_bias), out_weight)
    mixer_output = lax.psum_scatter(terms, "tp", scatter_dimension=0, tiled=True)
    expert_output = experts_half(
        expert_input,
        norm_gain,
        routes,
        route_weights,
        gate_weight,
        up_weight,
        down_weight,
        shared_gate,
        shared_up,
        shared_down,
    )
    return (mixer_output, expert_output)


def solution(mesh):
    placed = (
        P(("grp", "ep"), "tp"),
        P(("grp", "ep"), "tp", None),
        P("tp", ("grp", "ep")),
        P("tp", None),
        P(("grp", "ep", "tp"), None),
        P(),
        P(("grp", "ep", "tp"), None),
        P(("grp", "ep", "tp"), None),
        P(("ep", "tp"), None, None),
        P(("ep", "tp"), None, None),
        P(("ep", "tp"), None, None),
        P(),
        P(),
        P(),
    )
    return jax.shard_map(
        per_device,
        mesh=mesh,
        in_specs=placed,
        out_specs=(P(("grp", "ep", "tp"), None), P(("grp", "ep", "tp"), None)),
        check_vma=False,
    )
```

```python
import jax
import jax.numpy as jnp
from jax import lax
from jax.experimental import pallas as pl
from jax.experimental.pallas import tpu as pltpu
from jax.sharding import PartitionSpec as P

MESH = pl.DeviceIdType.MESH
F32 = jnp.float32
BF16 = jnp.bfloat16


def passed_along(block, axis, distance):
    devices = range(lax.axis_size(axis))
    route = [(i - distance, i) for i in devices if i - distance in devices]
    return lax.ppermute(block, axis, route)


def furthest_place(axis_size):
    chain_length = axis_size // max(1, axis_size // 4)
    return max(min((p + 2) % chain_length, p) for p in range(axis_size))


def attention_tile(q, k, v, bias, upper, kept, masked):
    z = lax.dot_general(q, k, (((1,), (1,)), ((), ())), preferred_element_type=F32) * 0.125 + bias
    tail = jnp.log(1.0 + jnp.exp(-jnp.abs(z)))
    log_sig = jnp.minimum(z, 0.0) - tail
    keep = -(jnp.maximum(z, 0.0) + tail)
    if masked:
        rows = lax.broadcasted_iota(jnp.int32, z.shape, 0)
        columns = lax.broadcasted_iota(jnp.int32, z.shape, 1)
        allowed = columns < rows
        keep = jnp.where(allowed, keep, 0.0)
    high = keep.astype(BF16)
    low = (keep - high.astype(F32)).astype(BF16)
    after = jnp.dot(high, upper, preferred_element_type=F32)
    after = after + jnp.dot(low, upper, preferred_element_type=F32)
    weight = jnp.exp(log_sig + after + kept)
    if masked:
        weight = jnp.where(allowed, weight, 0.0)
    part = jnp.dot(weight.astype(BF16), v, preferred_element_type=F32)
    return part, kept + jnp.sum(keep, axis=1, keepdims=True)


def attention_kernel(place_ref, q_ref, kv_ref, bias_ref, out_ref, total, kept):
    span, head_dim = q_ref.shape[1:]
    spans = kv_ref.shape[0]
    size = min(span, 256)
    tiles = span // size
    rows = lax.broadcasted_iota(jnp.int32, (size, size), 0)
    columns = lax.broadcasted_iota(jnp.int32, (size, size), 1)
    upper = jnp.where(rows > columns, 1.0, 0.0).astype(BF16)

    def tile(distance, i, j, masked, state):
        there = pl.ds(j * size, size)
        part, after = attention_tile(
            q_ref[0, i * size : (i + 1) * size, :],
            kv_ref[distance, 0, there, :head_dim],
            kv_ref[distance, 0, there, head_dim:],
            bias_ref[distance, 0, :, there].astype(F32),
            upper,
            state[1],
            masked,
        )
        return state[0] + part, after

    for i in range(tiles):
        state = (jnp.zeros((size, head_dim), F32), jnp.zeros((size, 1), F32))
        for j in range(i, -1, -1):
            state = tile(0, i, j, j == i, state)
        total[i] = state[0]
        kept[i] = jnp.broadcast_to(state[1], kept.shape[1:])
    for distance in range(1, spans):

        @pl.when(distance <= place_ref[0])
        def _():
            for i in range(tiles):
                state = (total[i], kept[i, :, :1])
                for j in range(tiles - 1, -1, -1):
                    state = tile(distance, i, j, False, state)
                total[i] = state[0]
                kept[i] = jnp.broadcast_to(state[1], kept.shape[1:])

    for i in range(tiles):
        out_ref[0, i * size : (i + 1) * size, :] = total[i].astype(out_ref.dtype)


def attend(queries, key_value, key_bias):
    span, key_groups, pair_width = key_value.shape
    head_dim = pair_width // 2
    heads = queries.shape[1] // head_dim
    per_group = heads // key_groups
    axis_size = lax.axis_size("ep")
    chain_length = axis_size // max(1, axis_size // 4)
    place = lax.axis_index("ep")
    chain_place = jnp.minimum((place + 2) % chain_length, place)
    furthest = furthest_place(axis_size)
    packed = jnp.concatenate([key_value.reshape(-1, pair_width), key_bias.reshape(-1, pair_width)])
    visiting = [packed]
    for _ in range(furthest):
        visiting.append(passed_along(visiting[-1], "ep", 1))
    visiting = jnp.stack(visiting)
    keys = visiting[:, : span * key_groups].reshape(-1, span, key_groups, pair_width)
    keys = keys.transpose(0, 2, 1, 3)
    biases = visiting[:, span * key_groups :].reshape(-1, key_groups, 1, span)
    size = min(span, 256)
    attended = pl.pallas_call(
        attention_kernel,
        grid=(heads,),
        out_shape=jax.ShapeDtypeStruct((heads, span, head_dim), BF16),
        in_specs=[
            pl.BlockSpec(memory_space=pltpu.SMEM),
            pl.BlockSpec((1, span, head_dim), lambda h: (h, 0, 0)),
            pl.BlockSpec((furthest + 1, 1, span, pair_width), lambda h: (0, h // per_group, 0, 0)),
            pl.BlockSpec((furthest + 1, 1, 1, span), lambda h: (0, h // per_group, 0, 0)),
        ],
        out_specs=pl.BlockSpec((1, span, head_dim), lambda h: (h, 0, 0)),
        scratch_shapes=[
            pltpu.VMEM((span // size, size, head_dim), F32),
            pltpu.VMEM((span // size, size, 128), F32),
        ],
        name="attention",
        cost_estimate=pl.CostEstimate(flops=4 * 10**9, bytes_accessed=10**6, transcendentals=0),
    )(
        chain_place.reshape(1),
        queries.reshape(span, heads, head_dim).transpose(1, 0, 2),
        keys,
        biases,
    )
    return attended.transpose(1, 0, 2).reshape(span, heads * head_dim)


def project(attended, out_weight):
    return jnp.dot(attended, out_weight, preferred_element_type=F32).astype(BF16)


def layer_kernel(
    capacity,
    q_ref,
    kv_ref,
    bias_ref,
    x_ref,
    gain_ref,
    routes_ref,
    route_weights_ref,
    out_weight_hbm,
    shared_gate_hbm,
    shared_up_hbm,
    shared_down_hbm,
    gate_hbm,
    up_hbm,
    down_hbm,
    mixer_ref,
    expert_ref,
    gathered,
    gathered_s,
    meta_out,
    meta,
    staged,
    staged_s,
    chosen,
    rows_in,
    rows_in_s,
    sums,
    sums_s,
    line_in,
    line_in_s,
    acc,
    acc_s,
    from_side,
    shared,
    out_weight_v,
    shared_gate_v,
    shared_up_v,
    shared_down_v,
    gate_v,
    up_v,
    down_v,
    kv_next,
    bias_row,
    bias_next,
    values_t,
    biases_t,
    att_total,
    att_kept,
    attended_t,
    terms,
    mixer_in,
    mixer_sum,
    mixer_side,
    load_sem,
    meta_send,
    meta_recv,
    kv_send,
    kv_recv,
    zs_send,
    zs_recv,
    s_send,
    s_recv,
    xa_send,
    xa_recv,
    xr_send,
    xr_recv,
    rz_send,
    rz_recv,
    last_send,
    last_recv,
    m_send,
    m_recv,
):
    count = lax.axis_size("ep")
    tokens, width = x_ref.shape
    columns, out_columns = piece_columns(width)
    pieces, out_pieces = len(columns), len(out_columns)
    cut, out_cut = columns[0].stop, out_columns[0].stop
    items, out_items = pieces + 1, out_pieces + 1
    z = lax.axis_index("ep")
    t = lax.axis_index("tp")
    x, c = t // 2, t % 2
    ox, oc = 1 - x, 1 - c
    places = (t, x * 2 + oc, ox * 2 + c, ox * 2 + oc)
    sibling, side = places[1], places[2]
    is_end = (z == 0) | (z == count - 1)

    def inside(zz):
        return (zz >= 0) & (zz < count)

    def copy(src, dst, send, recv, ep, tp):
        return pltpu.make_async_remote_copy(
            src_ref=src,
            dst_ref=dst,
            send_sem=send,
            recv_sem=recv,
            device_id={"ep": ep, "tp": tp},
            device_id_type=MESH,
        )

    def band(r):
        return slice(r * capacity, (r + 1) * capacity)

    loads = {
        name: pltpu.make_async_copy(a, b, load_sem.at[i])
        for i, (name, a, b) in enumerate(
            (
                ("shared_gate", shared_gate_hbm, shared_gate_v),
                ("shared_up", shared_up_hbm, shared_up_v),
                ("shared_down", shared_down_hbm, shared_down_v),
                ("gate", gate_hbm, gate_v),
                ("up", up_hbm, up_v),
                ("down", down_hbm, down_v),
                ("out_weight", out_weight_hbm, out_weight_v),
            )
        )
    }

    barrier = pltpu.get_barrier_semaphore()

    def greet(ep, tp):
        pl.semaphore_signal(barrier, 1, device_id={"ep": ep, "tp": tp}, device_id_type=MESH)

    for step in range(1, count):
        for sx in (0, 2):
            greet((z + step) % count, places[sx])
    for r in (1, 2, 3):
        greet(z, places[r])

    @pl.loop(0, tokens // 16)
    def _(block):
        rows = pl.ds(pl.multiple_of(block * 16, 16), 16)
        wide = x_ref[rows, :].astype(F32)
        mean = jnp.mean(wide * wide, axis=-1, keepdims=True)
        gathered[z, rows, :] = (wide * lax.rsqrt(mean + 1e-06) * gain_ref[...]).astype(BF16)

    lines = lax.broadcasted_iota(jnp.int32, (count * 8, tokens), 0)
    expert = (lines // 8) * 4 + lines % 4
    named = jnp.zeros((count * 8, tokens), F32)
    weight = jnp.zeros((count * 8, tokens), F32)
    for k in range(routes_ref.shape[0]):
        hit = routes_ref[k : k + 1, :] == expert
        named = named + jnp.where(hit, 1.0, 0.0)
        weight = weight + jnp.where(hit, route_weights_ref[k : k + 1, :], 0.0)
    before = lax.broadcasted_iota(jnp.int32, (tokens, tokens), 0) < lax.broadcasted_iota(
        jnp.int32, (tokens, tokens), 1
    )
    slot = jnp.dot(
        named.astype(BF16), jnp.where(before, 1.0, 0.0).astype(BF16), preferred_element_type=F32
    )
    slot = jnp.where(named > 0.5, slot, -1.0)
    meta_out[...] = jnp.where(lines % 8 < 4, slot, weight).reshape(meta_out.shape)
    meta[0, z] = meta_out[z]
    bias_row[...] = jnp.broadcast_to(bias_ref[...].astype(F32), bias_row.shape)

    pl.semaphore_wait(barrier, 2 * (count - 1) + 3)

    def meta_copy(step, sx):
        other = (z + step) % count
        return copy(
            meta_out.at[other],
            meta.at[sx, z],
            meta_send.at[sx, step],
            meta_recv.at[sx, z],
            other,
            places[2 * sx],
        )

    def meta_wait(sx, zz):
        copy(
            meta_out.at[zz], meta.at[sx, zz], meta_send.at[sx, 0], meta_recv.at[sx, zz], z, side
        ).wait_recv()

    def s_move():
        return copy(
            gathered.at[z, :, columns[0]], gathered_s.at[z], s_send.at[0], s_recv.at[0], z, side
        )

    def line(i, zz, item):
        small = 1 if item == pieces else 0
        block = gathered_s.at[zz] if small else gathered.at[zz, :, columns[item]]
        return copy(
            block, block, zs_send.at[i, small, zz], zs_recv.at[item, zz], z + 2 * i - 1, t
        )

    def kv_move(which):
        pair = ((kv_ref, kv_next), (bias_row, bias_next))[which]
        return copy(*pair, kv_send.at[which], kv_recv.at[which], z + 1, t)

    chain = count // max(1, count // 4)

    def chain_place(zz):
        return jnp.minimum((zz + 2) % chain, zz)

    sends_kv = (z + 1 < count) & (chain_place(z + 1) >= 1)
    takes_kv = chain_place(z) >= 1

    for step in range(1, count):
        for sx in range(2):
            meta_copy(step, sx).start()
    meta_copy(0, 1).start()
    s_move().start()
    for item in range(pieces):
        for i in range(2):

            @pl.when(inside(z + 2 * i - 1))
            def _():
                line(i, z, item).start()

    slots = lax.broadcasted_iota(jnp.int32, (capacity, tokens), 0).astype(F32)

    def one_hot(sx, zz, rels):
        return jnp.concatenate(
            [jnp.where(meta[sx, zz, pl.ds(places[r], 1), :] == slots, 1.0, 0.0) for r in rels],
            axis=0,
        ).astype(BF16)

    def spreader(sx, zz, rels):
        weights = jnp.concatenate(
            [
                jnp.where(
                    meta[sx, zz, pl.ds(places[r], 1), :] == slots,
                    meta[sx, zz, pl.ds(4 + places[r], 1), :],
                    0.0,
                )
                for r in rels
            ],
            axis=0,
        )
        high = weights.astype(BF16)
        return high, (weights - high.astype(F32)).astype(BF16)

    def spread(pair, rows):
        return sum(
            lax.dot_general(half, rows, (((0,), (0,)), ((), ())), preferred_element_type=F32)
            for half in pair
        )

    def row_copy(r, zz, p):
        if p == 0 and r == 3:
            return copy(
                staged_s.at[zz],
                chosen.at[zz, band(3), columns[0]],
                xa_send.at[r],
                xa_recv.at[r, zz],
                z,
                sibling,
            )
        return copy(
            staged.at[zz, band(r - 1), columns[p]],
            chosen.at[zz, band(r), columns[p]],
            xa_send.at[r],
            xa_recv.at[r, zz],
            z,
            places[r],
        )

    def pick(zz, p):
        rels = (0, 1) if p == 0 else (0, 1, 2, 3)
        picked = jnp.dot(
            one_hot(0, zz, rels), gathered[zz, :, columns[p]], preferred_element_type=F32
        ).astype(BF16)
        staged[zz, : (len(rels) - 1) * capacity, columns[p]] = picked[capacity:]
        chosen[zz, band(0), columns[p]] = picked[:capacity]
        for r in rels[:0:-1]:
            row_copy(r, zz, p).start()

    def pick_s(zz):
        picked = jnp.dot(
            one_hot(1, zz, (0, 1)), gathered_s[zz], preferred_element_type=F32
        ).astype(BF16)
        staged_s[zz] = picked[capacity:]
        chosen[zz, band(2), columns[0]] = picked[:capacity]
        row_copy(3, zz, 0).start()

    for p in (*range(1, pieces), 0):
        pick(z, p)
    s_move().wait_recv()
    for i in range(2):

        @pl.when(inside(z + 2 * i - 1))
        def _():
            line(i, z, pieces).start()

    @pl.when(sends_kv)
    def _():
        kv_move(1).start()
        kv_move(0).start()

    for load in loads.values():
        load.start()
    meta_wait(1, z)
    pick_s(z)

    span = kv_ref.shape[0]
    head_dim = kv_ref.shape[1] // 2
    heads = q_ref.shape[0] // head_dim
    size = min(span, 256)
    tiles = span // size
    key_line = lax.broadcasted_iota(jnp.int32, (size, size), 0)
    query_line = lax.broadcasted_iota(jnp.int32, (size, size), 1)

    def prepare(b, kv, bias):
        values_t[b] = kv[...].astype(F32).T[head_dim:, :].astype(BF16)
        biases_t[b] = jnp.broadcast_to(bias[0:1, :], (128, span)).T

    def tile(b, kv, h, i, j, state):
        there = slice(j * size, (j + 1) * size)
        diagonal = b == 0 and i == j
        later = jnp.where(key_line < query_line, 1.0, 0.0).astype(BF16)
        q = q_ref[pl.ds(pl.multiple_of(h * head_dim, head_dim), head_dim), i * size : (i + 1) * size]
        logits = jnp.dot(kv[there, :head_dim], q, preferred_element_type=F32) * 0.125
        logits = logits + biases_t[b, there, 0:1]
        log_sig = jnp.minimum(logits, 0.0) - jnp.log(1.0 + jnp.exp(-jnp.abs(logits)))
        keep = log_sig - logits
        if diagonal:
            keep = jnp.where(key_line < query_line, keep, 0.0)
        high = keep.astype(BF16)
        low = (keep - high.astype(F32)).astype(BF16)
        after = jnp.dot(later, high, preferred_element_type=F32)
        after = after + jnp.dot(later, low, preferred_element_type=F32)
        weights = jnp.exp(log_sig + after + state[1])
        if diagonal:
            weights = jnp.where(key_line < query_line, weights, 0.0)
        part = jnp.dot(values_t[b, :, there], weights.astype(BF16), preferred_element_type=F32)
        return state[0] + part, state[1] + jnp.sum(keep, axis=0, keepdims=True)

    def attend_own():
        prepare(0, kv_ref, bias_row)

        @pl.loop(0, heads)
        def _(h):
            for i in range(tiles):
                state = (jnp.zeros((head_dim, size), F32), jnp.zeros((1, size), F32))
                for j in range(i, -1, -1):
                    state = tile(0, kv_ref, h, i, j, state)
                att_total[h, i] = state[0]
                att_kept[h, i] = jnp.broadcast_to(state[1], att_kept.shape[2:])

    def attend_next(first, low, high):
        @pl.when(takes_kv)
        def _():
            if first:
                for which in range(2):
                    kv_move(which).wait_recv()
                prepare(1, kv_next, bias_next)

            @pl.loop(low, high)
            def _(h):
                for i in range(tiles):
                    state = (att_total[h, i], att_kept[h, i, 0:1, :])
                    for j in range(tiles - 1, -1, -1):
                        state = tile(1, kv_next, h, i, j, state)
                    att_total[h, i] = state[0]

    def mixer_pair(k):
        return copy(
            terms.at[3 - 2 * k], mixer_in.at[k], m_send.at[k], m_recv.at[k], z, sibling
        )

    def mixer_move():
        return copy(mixer_sum, mixer_side, m_send.at[2], m_recv.at[2], z, side)

    def project():
        for h in range(heads):
            for i in range(tiles):
                attended_t[h * head_dim : (h + 1) * head_dim, i * size : (i + 1) * size] = (
                    att_total[h, i].astype(BF16)
                )
        loads["out_weight"].wait()
        for r in (3, 1, 2, 0):
            own = pl.ds(pl.multiple_of(places[r] * tokens, tokens), tokens)
            terms[r] = lax.dot_general(
                attended_t[:, own],
                out_weight_v[...],
                (((0,), (0,)), ((), ())),
                preferred_element_type=F32,
            ).astype(BF16)
            if r % 2:
                mixer_pair((3 - r) // 2).start()
        mixer_pair(0).wait_recv()
        mixer_sum[...] = (terms[2].astype(F32) + mixer_in[0].astype(F32)).astype(BF16)

    def shared_expert():
        for name in ("shared_gate", "shared_up", "shared_down"):
            loads[name].wait()
        hidden_gate = jnp.dot(gathered[z], shared_gate_v[...], preferred_element_type=F32)
        hidden_up = jnp.dot(gathered[z], shared_up_v[...], preferred_element_type=F32)
        hidden = (hidden_gate / (1.0 + jnp.exp(-hidden_gate)) * hidden_up).astype(BF16)
        shared[...] = jnp.dot(hidden, shared_down_v[...], preferred_element_type=F32)

    def both(body):
        @pl.loop(0, 2)
        def _(i):
            body(i)

    def arrive(distance, item):
        def body(i):
            zz = z - (2 * i - 1) * distance

            @pl.when(inside(zz))
            def _():
                line(i, zz, item).wait_recv()

                @pl.when(inside(z + 2 * i - 1))
                def _():
                    line(i, zz, item).start()

                if item == 0:
                    meta_wait(0, zz)
                if item == pieces:
                    meta_wait(1, zz)
                    pick_s(zz)
                else:
                    pick(zz, item)

        both(body)

    def reach(r, start):
        return slice(start if r == 2 else 0, width)

    def result_copy(r, zz, p):
        if p == 0 and r == 3:
            destination, device = rows_in_s.at[zz, band(1)], sibling
        else:
            destination, device = rows_in.at[zz, band(r), out_columns[p]], places[r]
        return copy(
            chosen.at[zz, band(r), out_columns[p]],
            destination,
            xr_send.at[r],
            xr_recv.at[r, p, zz],
            z,
            device,
        )

    def crossing(p):
        return (1, 3) if p == 0 else (3, 2, 1)

    def send_results(zz, some=None):
        for p in some or range(out_pieces):
            for r in crossing(p):
                result_copy(r, zz, p).start()

    def feed_forward(zz, send):
        now = (out_pieces if send is True else send) if send else 0
        for r in (1, 2, 3):
            arrived = chosen.at[zz, band(r), reach(r, cut)]
            copy(arrived, arrived, xa_send.at[r], xa_recv.at[r, zz], z, sibling).wait_recv()
        gate = jnp.dot(chosen[zz], gate_v[...], preferred_element_type=F32)
        up = jnp.dot(chosen[zz], up_v[...], preferred_element_type=F32)
        hidden = (gate / (1.0 + jnp.exp(-gate)) * up).astype(BF16)
        for p in range(out_pieces):
            rows = jnp.dot(hidden, down_v[:, out_columns[p]], preferred_element_type=F32).astype(BF16)
            chosen[zz, :, out_columns[p]] = rows
            rows_in[zz, band(0), out_columns[p]] = rows[band(0)]
            if p == 0:
                rows_in_s[zz, band(0)] = rows[band(2)]


            if p < now:
                for r in crossing(p):
                    result_copy(r, zz, p).start()

    def planes_at(distance, act):
        def body(i):
            zz = z - (2 * i - 1) * distance

            @pl.when(inside(zz))
            def _():
                act(zz)

        both(body)

    def feed_forward_at(distance, send=True):
        planes_at(distance, lambda zz: feed_forward(zz, send))

    def back(i, target, item):
        if item == out_pieces:
            source, destination = sums_s.at[target], line_in_s.at[i, target]
        else:
            source = sums.at[target, :, out_columns[item]]
            destination = line_in.at[i, target, :, out_columns[item]]
        return copy(
            source,
            destination,
            rz_send.at[1 if item == out_pieces else 0, target],
            rz_recv.at[i, item, target],
            z + 2 * i - 1,
            t,
        )

    def total_of(zz, item):
        if item == out_pieces:
            result_copy(3, zz, 0).wait_recv()
            acc_s[...] = spread(spreader(1, zz, (0, 1)), rows_in_s[zz])
        elif item == 0:
            result_copy(1, zz, 0).wait_recv()
            acc[:, out_columns[0]] = spread(
                spreader(0, zz, (0, 1)), rows_in[zz, : 2 * capacity, out_columns[0]]
            )
        else:
            for r in crossing(item):
                result_copy(r, zz, item).wait_recv()
            acc[:, out_columns[item]] = spread(
                spreader(0, zz, (0, 1, 2, 3)), rows_in[zz, :, out_columns[item]]
            )

    def take_line(i, zz, item):
        back(i, zz, item).wait_recv()
        if item == out_pieces:
            acc_s[...] += line_in_s[i, zz].astype(F32)
        else:
            acc[:, out_columns[item]] += line_in[i, zz, :, out_columns[item]].astype(F32)

    item_order = (out_pieces, *range(out_pieces))

    near = jnp.where(2 * z < count, 1, 0)

    def stage_item(s, i, item):
        up = 2 * i - 1
        target = s * i + (count - 1 - s) * (1 - i)

        @pl.when(up * (target - z) > 0)
        def _():
            total_of(target, item)

            @pl.when(inside(z - up))
            def _():
                take_line(i, target, item)

            if item == out_pieces:
                sums_s[target] = acc_s[...].astype(BF16)
            else:
                sums[target, :, out_columns[item]] = acc[:, out_columns[item]].astype(BF16)
            back(i, target, item).start()

    def stage(s, aside=None):
        for k in range(out_items + 2):
            if k == 2 and aside:
                aside()
            if k < out_items:
                stage_item(s, near, item_order[k])
            if k >= 2:
                stage_item(s, 1 - near, item_order[k - 2])

    attend_own()
    early = {}
    for k in range(out_items):
        early.setdefault(min(k // 2 + 3, items - 1), []).append(k)
    arrive(1, 0)
    arrive(1, 1)
    shared_expert()
    for item in range(2, items):
        arrive(1, item)
    for name in ("gate", "up", "down"):
        loads[name].wait()
    feed_forward(z, False)
    for distance in range(2, count):
        last = distance == count - 1
        if not last:

            @pl.when(is_end)
            def _():
                if distance == 2:
                    send_results(z, (0, 1))
                feed_forward_at(distance - 1)

        for item in range(items):
            if last and item == 3:
                feed_forward_at(distance - 1, 3)

                @pl.when(jnp.logical_not(is_end))
                def _():
                    send_results(z)

            if distance == 2 and item in (2, 4):
                attend_next(item == 2, 0 if item == 2 else heads // 2, heads // 2 if item == 2 else heads - 1)
            if last and item == 2:
                attend_next(False, heads - 1, heads)
            arrive(distance, item)
            for k in early.get(item, ()) if distance == 2 and not last else ():
                stage_item(1, near, item_order[k])
        if not last:
            pl.when(jnp.logical_not(is_end))(lambda: feed_forward_at(distance - 1))
            if distance > 2:
                stage(distance - 1)
        elif 3 < out_pieces:
            planes_at(distance - 1, lambda zz: send_results(zz, tuple(range(3, out_pieces))))

    @pl.when(jnp.logical_not(is_end))
    def _():
        project()
        mixer_move().start()

    stage(count - 2)

    @pl.when(is_end)
    def _():
        send_results(z, (2, 3))

    feed_forward_at(count - 1)

    @pl.when(is_end)
    def _():
        send_results(z, (4, 5, 6))

    def mix_at_end():
        @pl.when(is_end)
        def _():
            project()
            mixer_move().start()

    stage(count - 1, mix_at_end)

    def last_move():
        return copy(sums_s.at[z], from_side, last_send.at[0], last_recv.at[0], z, side)

    def drain():
        for step in range(1, count):
            for sx in range(2):
                meta_copy(step, sx).wait_send()
        meta_copy(0, 1).wait_send()
        s_move().wait_send()

        @pl.when(sends_kv)
        def _():
            for which in range(2):
                kv_move(which).wait_send()

        for k in range(2):
            mixer_pair(k).wait_send()
        for r in (1, 2, 3):
            sent = staged.at[:, band(r - 1), reach(r, cut)]
            copy(sent, sent, xa_send.at[r], xa_recv.at[r, 0], z, sibling).wait_send()

        @pl.loop(0, count)
        def _(zz):
            for small in range(2):
                sent = (gathered, gathered_s)[small].at[zz]
                for i in range(2):
                    up = 2 * i - 1

                    @pl.when((up * (z - zz) >= 0) & inside(z + up))
                    def _():
                        copy(
                            sent, sent, zs_send.at[i, small, zz], zs_recv.at[0, zz], z, sibling
                        ).wait_send()

    for k, item in enumerate(item_order):
        if k == out_items // 2:
            drain()
        total_of(z, item)

        def body(i):
            @pl.when(inside(z - (2 * i - 1)))
            def _():
                take_line(i, z, item)

        both(body)
        if item == out_pieces:
            sums_s[z] = acc_s[...].astype(BF16)
            last_move().start()
        elif item > 0:
            expert_ref[:, out_columns[item]] = (
                acc[:, out_columns[item]] + shared[:, out_columns[item]]
            ).astype(BF16)

    for r in (1, 2, 3):
        sent = chosen.at[:, band(r), reach(r, out_cut)]
        copy(sent, sent, xr_send.at[r], xa_recv.at[r, 0], z, sibling).wait_send()

    @pl.loop(0, count)
    def _(zz):
        @pl.when(zz != z)
        def _():
            for small in range(2):
                sent = (sums, sums_s)[small].at[zz]
                copy(sent, sent, rz_send.at[small, zz], zs_recv.at[0, zz], z, sibling).wait_send()

    mixer_pair(1).wait_recv()
    mixer_move().wait_recv()
    mixer_ref[...] = (
        terms[0].astype(F32) + mixer_in[1].astype(F32) + mixer_side[...].astype(F32)
    ).astype(BF16)
    last_move().wait_recv()
    expert_ref[:, out_columns[0]] = (
        acc[:, out_columns[0]] + from_side[...].astype(F32) + shared[:, out_columns[0]]
    ).astype(BF16)
    mixer_move().wait_send()
    last_move().wait_send()


def piece_columns(width):
    unit = width // 16
    gather, result = ((0, 2, 5, 8, 10, 12, 14, 16), (0, 3, 5, 8, 10, 12, 14, 16))
    return tuple(
        [slice(a * unit, b * unit) for a, b in zip(edges, edges[1:])] for edges in (gather, result)
    )


def layer(
    queries,
    key_value,
    key_bias,
    out_weight,
    expert_input,
    norm_gain,
    routes,
    route_weights,
    routed_parts,
    shared_parts,
    capacity,
):
    tokens, width = expert_input.shape
    count = lax.axis_size("ep")
    columns, out_columns = piece_columns(width)
    cut, out_cut = columns[0].stop, out_columns[0].stop
    items, out_items = len(columns) + 1, len(out_columns) + 1
    span, _, pair_width = key_value.shape
    head_dim = pair_width // 2
    heads = queries.shape[1] // head_dim
    size = min(span, 256)
    hidden = routed_parts[0].shape[1]
    band = 4 * capacity
    dma = pltpu.SemaphoreType.DMA
    vmem = pl.BlockSpec(memory_space=pltpu.VMEM)
    hbm = pl.BlockSpec(memory_space=pl.ANY)
    buffers = [
        ((count, tokens, width), BF16),
        ((count, tokens, cut), BF16),
        ((count, 8, tokens), F32),
        ((2, count, 8, tokens), F32),
        ((count, 3 * capacity, width), BF16),
        ((count, capacity, cut), BF16),
        ((count, band, width), BF16),
        ((count, band, width), BF16),
        ((count, 2 * capacity, out_cut), BF16),
        ((count, tokens, width), BF16),
        ((count, tokens, out_cut), BF16),
        ((2, count, tokens, width), BF16),
        ((2, count, tokens, out_cut), BF16),
        ((tokens, width), F32),
        ((tokens, out_cut), F32),
        ((tokens, out_cut), BF16),
        ((tokens, width), F32),
        (out_weight.shape, BF16),
        (shared_parts[0].shape, BF16),
        (shared_parts[1].shape, BF16),
        (shared_parts[2].shape, BF16),
        ((width, hidden), BF16),
        ((width, hidden), BF16),
        ((hidden, width), BF16),
        ((span, pair_width), BF16),
        ((8, span), F32),
        ((8, span), F32),
        ((2, head_dim, span), BF16),
        ((2, span, 128), F32),
        ((heads, span // size, head_dim, size), F32),
        ((heads, span // size, 8, size), F32),
        ((heads * head_dim, span), BF16),
        ((4, tokens, width), BF16),
        ((2, tokens, width), BF16),
        ((tokens, width), BF16),
        ((tokens, width), BF16),
    ]
    semaphores = [
        (7,),
        (2, count),
        (2, count),
        (2,),
        (2,),
        (2, 2, count),
        (items, count),
        (1,),
        (1,),
        (4,),
        (4, count),
        (4,),
        (4, out_items - 1, count),
        (2, count),
        (2, out_items, count),
        (1,),
        (1,),
        (3,),
        (3,),
    ]
    return pl.pallas_call(
        lambda *refs: layer_kernel(capacity, *refs),
        out_shape=[pltpu.VMEM((tokens, width), BF16)] * 2,
        in_specs=[vmem] * 7 + [hbm] * 7,
        out_specs=[vmem] * 2,
        scratch_shapes=[pltpu.VMEM(*b) for b in buffers] + [dma(s) for s in semaphores],
        compiler_params=pltpu.CompilerParams(
            collective_id=0, has_side_effects=True, vmem_limit_bytes=60 * 2**20
        ),
        name="layer",
        cost_estimate=pl.CostEstimate(flops=10**10, bytes_accessed=2 * 10**7, transcendentals=0),
    )(
        queries.T,
        key_value.reshape(span, pair_width),
        key_bias,
        expert_input,
        norm_gain.reshape(1, width),
        routes.T,
        route_weights.T,
        out_weight,
        *shared_parts,
        *routed_parts,
    )


def expert_rows(arrived, gate_weight, up_weight, down_weight):
    sources, capacity, model_width = arrived.shape
    flat_rows = arrived.reshape(sources * capacity, model_width)
    gate_part = jnp.dot(flat_rows, gate_weight[0], preferred_element_type=jnp.float32)
    up_part = jnp.dot(flat_rows, up_weight[0], preferred_element_type=jnp.float32)
    hidden = (jax.nn.silu(gate_part) * up_part).astype(jnp.bfloat16)
    result = jnp.dot(hidden, down_weight[0], preferred_element_type=jnp.float32).astype(
        jnp.bfloat16
    )
    return result.reshape(sources, capacity, model_width)


def experts_half(
    expert_input,
    norm_gain,
    routes,
    route_weights,
    gate_weight,
    up_weight,
    down_weight,
    shared_gate,
    shared_up,
    shared_down,
):
    tokens, top_count = routes.shape
    model_width = expert_input.shape[1]
    ep_count = lax.axis_size("ep")
    tp_count = lax.axis_size("tp")
    experts = ep_count * tp_count
    capacity = max(2, 3 * tokens * top_count // (2 * experts))
    widened = expert_input.astype(jnp.float32)
    normed = (
        widened * lax.rsqrt(jnp.mean(widened * widened, axis=-1, keepdims=True) + 1e-06) * norm_gain
    ).astype(jnp.bfloat16)
    flat_routes = routes.reshape(-1)
    one_hot = (flat_routes[:, None] == jnp.arange(experts, dtype=jnp.int32)[None, :]).astype(
        jnp.int32
    )
    before = jnp.cumsum(one_hot, axis=0) - one_hot
    slot_index = jnp.sum(before * one_hot, axis=1)
    target = flat_routes * capacity + slot_index
    picker = (jnp.arange(experts * capacity, dtype=jnp.int32)[:, None] == target[None, :]).astype(
        jnp.bfloat16
    )
    picker = jnp.sum(picker.reshape(experts * capacity, tokens, top_count), axis=2)
    outgoing = jnp.dot(picker, normed, preferred_element_type=jnp.float32).astype(jnp.bfloat16)
    outgoing = outgoing.reshape(experts, capacity, model_width)
    came_back = lax.all_to_all(
        expert_rows(
            lax.all_to_all(outgoing, ("ep", "tp"), split_axis=0, concat_axis=0, tiled=True),
            gate_weight,
            up_weight,
            down_weight,
        ),
        ("ep", "tp"),
        split_axis=0,
        concat_axis=0,
        tiled=True,
    )
    back_rows = came_back.reshape(experts * capacity, model_width)
    picked = jnp.take(back_rows, target, axis=0).reshape(tokens, top_count, model_width)
    routed = jnp.sum(picked.astype(jnp.float32) * route_weights[:, :, None], axis=1)
    shared_hidden = (
        jax.nn.silu(jnp.dot(normed, shared_gate, preferred_element_type=jnp.float32))
        * jnp.dot(normed, shared_up, preferred_element_type=jnp.float32)
    ).astype(jnp.bfloat16)
    shared_term = jnp.dot(shared_hidden, shared_down, preferred_element_type=jnp.float32)
    return (routed + shared_term).astype(jnp.bfloat16)


def per_device(
    queries,
    key_value,
    key_bias,
    out_weight,
    expert_input,
    norm_gain,
    routes,
    route_weights,
    gate_weight,
    up_weight,
    down_weight,
    shared_gate,
    shared_up,
    shared_down,
):
    tokens, top_count = routes.shape
    span, key_groups, pair_width = key_value.shape
    width = expert_input.shape[1]
    ep_count, tp_count = lax.axis_size("ep"), lax.axis_size("tp")
    experts = ep_count * tp_count
    capacity = max(2, 3 * tokens * top_count // (2 * experts))
    fits = experts * tokens * width * 2 <= 8 * 2**20 and capacity % 16 == 0 and ep_count >= 3
    whole = tp_count == 4 and span == tp_count * tokens and tokens == 128
    heads_fit = key_groups == 1 and pair_width == 128 and width % 1024 == 0
    if fits and whole and heads_fit and furthest_place(ep_count) <= 1:
        return tuple(
            layer(
                queries,
                key_value,
                key_bias,
                out_weight,
                expert_input,
                norm_gain,
                routes,
                route_weights,
                (gate_weight[0], up_weight[0], down_weight[0]),
                (shared_gate, shared_up, shared_down),
                capacity,
            )
        )
    terms = project(attend(queries, key_value, key_bias), out_weight)
    mixer_output = lax.psum_scatter(terms, "tp", scatter_dimension=0, tiled=True)
    expert_output = experts_half(
        expert_input,
        norm_gain,
        routes,
        route_weights,
        gate_weight,
        up_weight,
        down_weight,
        shared_gate,
        shared_up,
        shared_down,
    )
    return (mixer_output, expert_output)


def solution(mesh):
    placed = (
        P(("grp", "ep"), "tp"),
        P(("grp", "ep"), "tp", None),
        P("tp", ("grp", "ep")),
        P("tp", None),
        P(("grp", "ep", "tp"), None),
        P(),
        P(("grp", "ep", "tp"), None),
        P(("grp", "ep", "tp"), None),
        P(("ep", "tp"), None, None),
        P(("ep", "tp"), None, None),
        P(("ep", "tp"), None, None),
        P(),
        P(),
        P(),
    )
    return jax.shard_map(
        per_device,
        mesh=mesh,
        in_specs=placed,
        out_specs=(P(("grp", "ep", "tp"), None), P(("grp", "ep", "tp"), None)),
        check_vma=False,
    )
```

```python
import jax
import jax.numpy as jnp
from jax import lax
from jax.experimental import pallas as pl
from jax.experimental.pallas import tpu as pltpu
from jax.sharding import PartitionSpec as P

MESH = pl.DeviceIdType.MESH
F32 = jnp.float32
BF16 = jnp.bfloat16


def passed_along(block, axis, distance):
    devices = range(lax.axis_size(axis))
    route = [(i - distance, i) for i in devices if i - distance in devices]
    return lax.ppermute(block, axis, route)


def furthest_place(axis_size):
    chain_length = axis_size // max(1, axis_size // 4)
    return max(min((p + 2) % chain_length, p) for p in range(axis_size))


def attention_tile(q, k, v, bias, upper, kept, masked):
    z = lax.dot_general(q, k, (((1,), (1,)), ((), ())), preferred_element_type=F32) * 0.125 + bias
    tail = jnp.log(1.0 + jnp.exp(-jnp.abs(z)))
    log_sig = jnp.minimum(z, 0.0) - tail
    keep = -(jnp.maximum(z, 0.0) + tail)
    if masked:
        rows = lax.broadcasted_iota(jnp.int32, z.shape, 0)
        columns = lax.broadcasted_iota(jnp.int32, z.shape, 1)
        allowed = columns < rows
        keep = jnp.where(allowed, keep, 0.0)
    high = keep.astype(BF16)
    low = (keep - high.astype(F32)).astype(BF16)
    after = jnp.dot(high, upper, preferred_element_type=F32)
    after = after + jnp.dot(low, upper, preferred_element_type=F32)
    weight = jnp.exp(log_sig + after + kept)
    if masked:
        weight = jnp.where(allowed, weight, 0.0)
    part = jnp.dot(weight.astype(BF16), v, preferred_element_type=F32)
    return part, kept + jnp.sum(keep, axis=1, keepdims=True)


def attention_kernel(place_ref, q_ref, kv_ref, bias_ref, out_ref, total, kept):
    span, head_dim = q_ref.shape[1:]
    spans = kv_ref.shape[0]
    size = min(span, 256)
    tiles = span // size
    rows = lax.broadcasted_iota(jnp.int32, (size, size), 0)
    columns = lax.broadcasted_iota(jnp.int32, (size, size), 1)
    upper = jnp.where(rows > columns, 1.0, 0.0).astype(BF16)

    def tile(distance, i, j, masked, state):
        there = pl.ds(j * size, size)
        part, after = attention_tile(
            q_ref[0, i * size : (i + 1) * size, :],
            kv_ref[distance, 0, there, :head_dim],
            kv_ref[distance, 0, there, head_dim:],
            bias_ref[distance, 0, :, there].astype(F32),
            upper,
            state[1],
            masked,
        )
        return state[0] + part, after

    for i in range(tiles):
        state = (jnp.zeros((size, head_dim), F32), jnp.zeros((size, 1), F32))
        for j in range(i, -1, -1):
            state = tile(0, i, j, j == i, state)
        total[i] = state[0]
        kept[i] = jnp.broadcast_to(state[1], kept.shape[1:])
    for distance in range(1, spans):

        @pl.when(distance <= place_ref[0])
        def _():
            for i in range(tiles):
                state = (total[i], kept[i, :, :1])
                for j in range(tiles - 1, -1, -1):
                    state = tile(distance, i, j, False, state)
                total[i] = state[0]
                kept[i] = jnp.broadcast_to(state[1], kept.shape[1:])

    for i in range(tiles):
        out_ref[0, i * size : (i + 1) * size, :] = total[i].astype(out_ref.dtype)


def attend(queries, key_value, key_bias):
    span, key_groups, pair_width = key_value.shape
    head_dim = pair_width // 2
    heads = queries.shape[1] // head_dim
    per_group = heads // key_groups
    axis_size = lax.axis_size("ep")
    chain_length = axis_size // max(1, axis_size // 4)
    place = lax.axis_index("ep")
    chain_place = jnp.minimum((place + 2) % chain_length, place)
    furthest = furthest_place(axis_size)
    packed = jnp.concatenate([key_value.reshape(-1, pair_width), key_bias.reshape(-1, pair_width)])
    visiting = [packed]
    for _ in range(furthest):
        visiting.append(passed_along(visiting[-1], "ep", 1))
    visiting = jnp.stack(visiting)
    keys = visiting[:, : span * key_groups].reshape(-1, span, key_groups, pair_width)
    keys = keys.transpose(0, 2, 1, 3)
    biases = visiting[:, span * key_groups :].reshape(-1, key_groups, 1, span)
    size = min(span, 256)
    attended = pl.pallas_call(
        attention_kernel,
        grid=(heads,),
        out_shape=jax.ShapeDtypeStruct((heads, span, head_dim), BF16),
        in_specs=[
            pl.BlockSpec(memory_space=pltpu.SMEM),
            pl.BlockSpec((1, span, head_dim), lambda h: (h, 0, 0)),
            pl.BlockSpec((furthest + 1, 1, span, pair_width), lambda h: (0, h // per_group, 0, 0)),
            pl.BlockSpec((furthest + 1, 1, 1, span), lambda h: (0, h // per_group, 0, 0)),
        ],
        out_specs=pl.BlockSpec((1, span, head_dim), lambda h: (h, 0, 0)),
        scratch_shapes=[
            pltpu.VMEM((span // size, size, head_dim), F32),
            pltpu.VMEM((span // size, size, 128), F32),
        ],
        name="attention",
        cost_estimate=pl.CostEstimate(flops=4 * 10**9, bytes_accessed=10**6, transcendentals=0),
    )(
        chain_place.reshape(1),
        queries.reshape(span, heads, head_dim).transpose(1, 0, 2),
        keys,
        biases,
    )
    return attended.transpose(1, 0, 2).reshape(span, heads * head_dim)


def project(attended, out_weight):
    return jnp.dot(attended, out_weight, preferred_element_type=F32).astype(BF16)


def layer_kernel(
    capacity,
    q_ref,
    kv_ref,
    bias_ref,
    x_ref,
    gain_ref,
    routes_ref,
    route_weights_ref,
    out_weight_hbm,
    shared_gate_hbm,
    shared_up_hbm,
    shared_down_hbm,
    gate_hbm,
    up_hbm,
    down_hbm,
    mixer_ref,
    expert_ref,
    gathered,
    gathered_s,
    meta_out,
    meta,
    staged,
    staged_s,
    chosen,
    rows_in,
    rows_in_s,
    sums,
    sums_s,
    line_in,
    line_in_s,
    acc,
    acc_s,
    from_side,
    shared,
    out_weight_v,
    shared_gate_v,
    shared_up_v,
    shared_down_v,
    gate_v,
    up_v,
    down_v,
    kv_next,
    bias_row,
    bias_next,
    values_t,
    biases_t,
    att_total,
    att_kept,
    attended_t,
    terms,
    mixer_in,
    mixer_sum,
    mixer_side,
    load_sem,
    meta_send,
    meta_recv,
    kv_send,
    kv_recv,
    zs_send,
    zs_recv,
    s_send,
    s_recv,
    xa_send,
    xa_recv,
    xr_send,
    xr_recv,
    rz_send,
    rz_recv,
    last_send,
    last_recv,
    m_send,
    m_recv,
):
    count = lax.axis_size("ep")
    tokens, width = x_ref.shape
    columns, out_columns = piece_columns(width)
    pieces, out_pieces = len(columns), len(out_columns)
    cut, out_cut = columns[0].stop, out_columns[0].stop
    items, out_items = pieces + 1, out_pieces + 1
    z = lax.axis_index("ep")
    t = lax.axis_index("tp")
    x, c = t // 2, t % 2
    ox, oc = 1 - x, 1 - c
    places = (t, x * 2 + oc, ox * 2 + c, ox * 2 + oc)
    sibling, side = places[1], places[2]
    is_end = (z == 0) | (z == count - 1)

    def inside(zz):
        return (zz >= 0) & (zz < count)

    def copy(src, dst, send, recv, ep, tp):
        return pltpu.make_async_remote_copy(
            src_ref=src,
            dst_ref=dst,
            send_sem=send,
            recv_sem=recv,
            device_id={"ep": ep, "tp": tp},
            device_id_type=MESH,
        )

    def band(r):
        return slice(r * capacity, (r + 1) * capacity)

    loads = {
        name: pltpu.make_async_copy(a, b, load_sem.at[i])
        for i, (name, a, b) in enumerate(
            (
                ("shared_gate", shared_gate_hbm, shared_gate_v),
                ("shared_up", shared_up_hbm, shared_up_v),
                ("shared_down", shared_down_hbm, shared_down_v),
                ("gate", gate_hbm, gate_v),
                ("up", up_hbm, up_v),
                ("down", down_hbm, down_v),
                ("out_weight", out_weight_hbm, out_weight_v),
            )
        )
    }

    barrier = pltpu.get_barrier_semaphore()

    def greet(ep, tp):
        pl.semaphore_signal(barrier, 1, device_id={"ep": ep, "tp": tp}, device_id_type=MESH)

    for step in range(1, count):
        for sx in (0, 2):
            greet((z + step) % count, places[sx])
    for r in (1, 2, 3):
        greet(z, places[r])

    @pl.loop(0, tokens // 16)
    def _(block):
        rows = pl.ds(pl.multiple_of(block * 16, 16), 16)
        wide = x_ref[rows, :].astype(F32)
        mean = jnp.mean(wide * wide, axis=-1, keepdims=True)
        gathered[z, rows, :] = (wide * lax.rsqrt(mean + 1e-06) * gain_ref[...]).astype(BF16)

    lines = lax.broadcasted_iota(jnp.int32, (count * 8, tokens), 0)
    expert = (lines // 8) * 4 + lines % 4
    named = jnp.zeros((count * 8, tokens), F32)
    weight = jnp.zeros((count * 8, tokens), F32)
    for k in range(routes_ref.shape[0]):
        hit = routes_ref[k : k + 1, :] == expert
        named = named + jnp.where(hit, 1.0, 0.0)
        weight = weight + jnp.where(hit, route_weights_ref[k : k + 1, :], 0.0)
    before = lax.broadcasted_iota(jnp.int32, (tokens, tokens), 0) < lax.broadcasted_iota(
        jnp.int32, (tokens, tokens), 1
    )
    slot = jnp.dot(
        named.astype(BF16), jnp.where(before, 1.0, 0.0).astype(BF16), preferred_element_type=F32
    )
    slot = jnp.where(named > 0.5, slot, -1.0)
    meta_out[...] = jnp.where(lines % 8 < 4, slot, weight).reshape(meta_out.shape)
    meta[0, z] = meta_out[z]
    bias_row[...] = jnp.broadcast_to(bias_ref[...].astype(F32), bias_row.shape)

    pl.semaphore_wait(barrier, 2 * (count - 1) + 3)

    def meta_copy(step, sx):
        other = (z + step) % count
        return copy(
            meta_out.at[other],
            meta.at[sx, z],
            meta_send.at[sx, step],
            meta_recv.at[sx, z],
            other,
            places[2 * sx],
        )

    def meta_wait(sx, zz):
        copy(
            meta_out.at[zz], meta.at[sx, zz], meta_send.at[sx, 0], meta_recv.at[sx, zz], z, side
        ).wait_recv()

    def s_move():
        return copy(
            gathered.at[z, :, columns[0]], gathered_s.at[z], s_send.at[0], s_recv.at[0], z, side
        )

    def line(i, zz, item):
        small = 1 if item == pieces else 0
        block = gathered_s.at[zz] if small else gathered.at[zz, :, columns[item]]
        return copy(
            block, block, zs_send.at[i, small, zz], zs_recv.at[item, zz], z + 2 * i - 1, t
        )

    def kv_move(which):
        pair = ((kv_ref, kv_next), (bias_row, bias_next))[which]
        return copy(*pair, kv_send.at[which], kv_recv.at[which], z + 1, t)

    chain = count // max(1, count // 4)

    def chain_place(zz):
        return jnp.minimum((zz + 2) % chain, zz)

    sends_kv = (z + 1 < count) & (chain_place(z + 1) >= 1)
    takes_kv = chain_place(z) >= 1

    for step in range(1, count):
        for sx in range(2):
            meta_copy(step, sx).start()
    meta_copy(0, 1).start()
    s_move().start()
    for item in range(pieces):
        for i in range(2):

            @pl.when(inside(z + 2 * i - 1))
            def _():
                line(i, z, item).start()

    slots = lax.broadcasted_iota(jnp.int32, (capacity, tokens), 0).astype(F32)

    def one_hot(sx, zz, rels):
        return jnp.concatenate(
            [jnp.where(meta[sx, zz, pl.ds(places[r], 1), :] == slots, 1.0, 0.0) for r in rels],
            axis=0,
        ).astype(BF16)

    def spreader(sx, zz, rels):
        weights = jnp.concatenate(
            [
                jnp.where(
                    meta[sx, zz, pl.ds(places[r], 1), :] == slots,
                    meta[sx, zz, pl.ds(4 + places[r], 1), :],
                    0.0,
                )
                for r in rels
            ],
            axis=0,
        )
        high = weights.astype(BF16)
        return high, (weights - high.astype(F32)).astype(BF16)

    def spread(pair, rows):
        return sum(
            lax.dot_general(half, rows, (((0,), (0,)), ((), ())), preferred_element_type=F32)
            for half in pair
        )

    def row_copy(r, zz, p):
        if p == 0 and r == 3:
            return copy(
                staged_s.at[zz],
                chosen.at[zz, band(3), columns[0]],
                xa_send.at[r],
                xa_recv.at[r, zz],
                z,
                sibling,
            )
        return copy(
            staged.at[zz, band(r - 1), columns[p]],
            chosen.at[zz, band(r), columns[p]],
            xa_send.at[r],
            xa_recv.at[r, zz],
            z,
            places[r],
        )

    def pick(zz, p):
        rels = (0, 1) if p == 0 else (0, 1, 2, 3)
        picked = jnp.dot(
            one_hot(0, zz, rels), gathered[zz, :, columns[p]], preferred_element_type=F32
        ).astype(BF16)
        staged[zz, : (len(rels) - 1) * capacity, columns[p]] = picked[capacity:]
        chosen[zz, band(0), columns[p]] = picked[:capacity]
        for r in rels[:0:-1]:
            row_copy(r, zz, p).start()

    def pick_s(zz):
        picked = jnp.dot(
            one_hot(1, zz, (0, 1)), gathered_s[zz], preferred_element_type=F32
        ).astype(BF16)
        staged_s[zz] = picked[capacity:]
        chosen[zz, band(2), columns[0]] = picked[:capacity]
        row_copy(3, zz, 0).start()

    for p in (*range(1, pieces), 0):
        pick(z, p)
    s_move().wait_recv()
    for i in range(2):

        @pl.when(inside(z + 2 * i - 1))
        def _():
            line(i, z, pieces).start()

    @pl.when(sends_kv)
    def _():
        kv_move(1).start()
        kv_move(0).start()

    for load in loads.values():
        load.start()
    meta_wait(1, z)
    pick_s(z)

    span = kv_ref.shape[0]
    head_dim = kv_ref.shape[1] // 2
    heads = q_ref.shape[0] // head_dim
    size = min(span, 256)
    tiles = span // size
    key_line = lax.broadcasted_iota(jnp.int32, (size, size), 0)
    query_line = lax.broadcasted_iota(jnp.int32, (size, size), 1)

    def prepare(b, kv, bias):
        values_t[b] = kv[...].astype(F32).T[head_dim:, :].astype(BF16)
        biases_t[b] = jnp.broadcast_to(bias[0:1, :], (128, span)).T

    def tile(b, kv, h, i, j, state):
        there = slice(j * size, (j + 1) * size)
        diagonal = b == 0 and i == j
        later = jnp.where(key_line < query_line, 1.0, 0.0).astype(BF16)
        q = q_ref[pl.ds(pl.multiple_of(h * head_dim, head_dim), head_dim), i * size : (i + 1) * size]
        logits = jnp.dot(kv[there, :head_dim], q, preferred_element_type=F32) * 0.125
        logits = logits + biases_t[b, there, 0:1]
        log_sig = jnp.minimum(logits, 0.0) - jnp.log(1.0 + jnp.exp(-jnp.abs(logits)))
        keep = log_sig - logits
        if diagonal:
            keep = jnp.where(key_line < query_line, keep, 0.0)
        high = keep.astype(BF16)
        low = (keep - high.astype(F32)).astype(BF16)
        after = jnp.dot(later, high, preferred_element_type=F32)
        after = after + jnp.dot(later, low, preferred_element_type=F32)
        weights = jnp.exp(log_sig + after + state[1])
        if diagonal:
            weights = jnp.where(key_line < query_line, weights, 0.0)
        part = jnp.dot(values_t[b, :, there], weights.astype(BF16), preferred_element_type=F32)
        return state[0] + part, state[1] + jnp.sum(keep, axis=0, keepdims=True)

    def attend_own():
        prepare(0, kv_ref, bias_row)

        @pl.loop(0, heads)
        def _(h):
            for i in range(tiles):
                state = (jnp.zeros((head_dim, size), F32), jnp.zeros((1, size), F32))
                for j in range(i, -1, -1):
                    state = tile(0, kv_ref, h, i, j, state)
                att_total[h, i] = state[0]
                att_kept[h, i] = jnp.broadcast_to(state[1], att_kept.shape[2:])

    def attend_next(first, low, high):
        @pl.when(takes_kv)
        def _():
            if first:
                for which in range(2):
                    kv_move(which).wait_recv()
                prepare(1, kv_next, bias_next)

            @pl.loop(low, high)
            def _(h):
                for i in range(tiles):
                    state = (att_total[h, i], att_kept[h, i, 0:1, :])
                    for j in range(tiles - 1, -1, -1):
                        state = tile(1, kv_next, h, i, j, state)
                    att_total[h, i] = state[0]

    def mixer_pair(k):
        return copy(
            terms.at[3 - 2 * k], mixer_in.at[k], m_send.at[k], m_recv.at[k], z, sibling
        )

    def mixer_move():
        return copy(mixer_sum, mixer_side, m_send.at[2], m_recv.at[2], z, side)

    def project():
        for h in range(heads):
            for i in range(tiles):
                attended_t[h * head_dim : (h + 1) * head_dim, i * size : (i + 1) * size] = (
                    att_total[h, i].astype(BF16)
                )
        loads["out_weight"].wait()
        for r in (3, 1, 2, 0):
            own = pl.ds(pl.multiple_of(places[r] * tokens, tokens), tokens)
            terms[r] = lax.dot_general(
                attended_t[:, own],
                out_weight_v[...],
                (((0,), (0,)), ((), ())),
                preferred_element_type=F32,
            ).astype(BF16)
            if r % 2:
                mixer_pair((3 - r) // 2).start()
        mixer_pair(0).wait_recv()
        mixer_sum[...] = (terms[2].astype(F32) + mixer_in[0].astype(F32)).astype(BF16)

    def shared_expert():
        for name in ("shared_gate", "shared_up", "shared_down"):
            loads[name].wait()
        hidden_gate = jnp.dot(gathered[z], shared_gate_v[...], preferred_element_type=F32)
        hidden_up = jnp.dot(gathered[z], shared_up_v[...], preferred_element_type=F32)
        hidden = (hidden_gate / (1.0 + jnp.exp(-hidden_gate)) * hidden_up).astype(BF16)
        shared[...] = jnp.dot(hidden, shared_down_v[...], preferred_element_type=F32)

    def both(body):
        @pl.loop(0, 2)
        def _(i):
            body(i)

    def arrive(distance, item):
        def body(i):
            zz = z - (2 * i - 1) * distance

            @pl.when(inside(zz))
            def _():
                line(i, zz, item).wait_recv()

                @pl.when(inside(z + 2 * i - 1))
                def _():
                    line(i, zz, item).start()

                if item == 0:
                    meta_wait(0, zz)
                if item == pieces:
                    meta_wait(1, zz)
                    pick_s(zz)
                else:
                    pick(zz, item)

        both(body)

    def reach(r, start):
        return slice(start if r == 2 else 0, width)

    def result_copy(r, zz, p):
        if p == 0 and r == 3:
            destination, device = rows_in_s.at[zz, band(1)], sibling
        else:
            destination, device = rows_in.at[zz, band(r), out_columns[p]], places[r]
        return copy(
            chosen.at[zz, band(r), out_columns[p]],
            destination,
            xr_send.at[r],
            xr_recv.at[r, p, zz],
            z,
            device,
        )

    def crossing(p):
        return (1, 3) if p == 0 else (3, 2, 1)

    def send_results(zz, some=None):
        for p in some or range(out_pieces):
            for r in crossing(p):
                result_copy(r, zz, p).start()

    def feed_forward(zz, send):
        now = (out_pieces if send is True else send) if send else 0
        for r in (1, 2, 3):
            arrived = chosen.at[zz, band(r), reach(r, cut)]
            copy(arrived, arrived, xa_send.at[r], xa_recv.at[r, zz], z, sibling).wait_recv()
        gate = jnp.dot(chosen[zz], gate_v[...], preferred_element_type=F32)
        up = jnp.dot(chosen[zz], up_v[...], preferred_element_type=F32)
        hidden = (gate / (1.0 + jnp.exp(-gate)) * up).astype(BF16)
        for p in range(out_pieces):
            rows = jnp.dot(hidden, down_v[:, out_columns[p]], preferred_element_type=F32).astype(BF16)
            chosen[zz, :, out_columns[p]] = rows
            rows_in[zz, band(0), out_columns[p]] = rows[band(0)]
            if p == 0:
                rows_in_s[zz, band(0)] = rows[band(2)]


            if p < now:
                for r in crossing(p):
                    result_copy(r, zz, p).start()

    def planes_at(distance, act):
        def body(i):
            zz = z - (2 * i - 1) * distance

            @pl.when(inside(zz))
            def _():
                act(zz)

        both(body)

    def feed_forward_at(distance, send=True):
        planes_at(distance, lambda zz: feed_forward(zz, send))

    def back(i, target, item):
        if item == out_pieces:
            source, destination = sums_s.at[target], line_in_s.at[i, target]
        else:
            source = sums.at[target, :, out_columns[item]]
            destination = line_in.at[i, target, :, out_columns[item]]
        return copy(
            source,
            destination,
            rz_send.at[1 if item == out_pieces else 0, target],
            rz_recv.at[i, item, target],
            z + 2 * i - 1,
            t,
        )

    def total_of(zz, item):
        if item == out_pieces:
            result_copy(3, zz, 0).wait_recv()
            acc_s[...] = spread(spreader(1, zz, (0, 1)), rows_in_s[zz])
        elif item == 0:
            result_copy(1, zz, 0).wait_recv()
            acc[:, out_columns[0]] = spread(
                spreader(0, zz, (0, 1)), rows_in[zz, : 2 * capacity, out_columns[0]]
            )
        else:
            for r in crossing(item):
                result_copy(r, zz, item).wait_recv()
            acc[:, out_columns[item]] = spread(
                spreader(0, zz, (0, 1, 2, 3)), rows_in[zz, :, out_columns[item]]
            )

    def take_line(i, zz, item):
        back(i, zz, item).wait_recv()
        if item == out_pieces:
            acc_s[...] += line_in_s[i, zz].astype(F32)
        else:
            acc[:, out_columns[item]] += line_in[i, zz, :, out_columns[item]].astype(F32)

    item_order = (out_pieces, *range(out_pieces))

    near = jnp.where(2 * z < count, 1, 0)

    def stage_item(s, i, item):
        up = 2 * i - 1
        target = s * i + (count - 1 - s) * (1 - i)

        @pl.when(up * (target - z) > 0)
        def _():
            total_of(target, item)

            @pl.when(inside(z - up))
            def _():
                take_line(i, target, item)

            if item == out_pieces:
                sums_s[target] = acc_s[...].astype(BF16)
            else:
                sums[target, :, out_columns[item]] = acc[:, out_columns[item]].astype(BF16)
            back(i, target, item).start()

    def stage(s, aside=None, moment=2):
        for k in range(out_items + 2):
            if k == moment and aside:
                aside()
            if k < out_items:
                stage_item(s, near, item_order[k])
            if k >= 2:
                stage_item(s, 1 - near, item_order[k - 2])

    attend_own()
    early = {}
    for k in range(out_items):
        early.setdefault(min(k // 2 + 3, items - 1), []).append(k)
    arrive(1, 0)
    arrive(1, 1)
    shared_expert()
    for item in range(2, items):
        arrive(1, item)
    for name in ("gate", "up", "down"):
        loads[name].wait()
    feed_forward(z, False)
    for distance in range(2, count):
        last = distance == count - 1
        if not last:

            @pl.when(is_end)
            def _():
                if distance == 2:
                    send_results(z, (0, 1))
                feed_forward_at(distance - 1)

        for item in range(items):
            if last and item == 3:
                feed_forward_at(distance - 1, 4)

            if distance == 2 and item in (2, 4):
                attend_next(item == 2, 0 if item == 2 else heads // 2, heads // 2 if item == 2 else heads - 1)
            if last and item == 2:
                attend_next(False, heads - 1, heads)
            arrive(distance, item)
            for k in early.get(item, ()) if distance == 2 and not last else ():
                stage_item(1, near, item_order[k])
        if not last:
            pl.when(jnp.logical_not(is_end))(lambda: feed_forward_at(distance - 1))
            if distance > 2:
                stage(distance - 1)
        elif 4 < out_pieces:
            planes_at(distance - 1, lambda zz: send_results(zz, tuple(range(4, out_pieces))))

    @pl.when(jnp.logical_not(is_end))
    def _():
        send_results(z)
        project()
        mixer_move().start()

    stage(count - 2, lambda: feed_forward_at(count - 1), 5)

    @pl.when(is_end)
    def _():
        send_results(z, (2, 3, 4, 5, 6))

    def mix_at_end():
        @pl.when(is_end)
        def _():
            project()
            mixer_move().start()

    stage(count - 1, mix_at_end)

    def last_move():
        return copy(sums_s.at[z], from_side, last_send.at[0], last_recv.at[0], z, side)

    def drain():
        for step in range(1, count):
            for sx in range(2):
                meta_copy(step, sx).wait_send()
        meta_copy(0, 1).wait_send()
        s_move().wait_send()

        @pl.when(sends_kv)
        def _():
            for which in range(2):
                kv_move(which).wait_send()

        for k in range(2):
            mixer_pair(k).wait_send()
        for r in (1, 2, 3):
            sent = staged.at[:, band(r - 1), reach(r, cut)]
            copy(sent, sent, xa_send.at[r], xa_recv.at[r, 0], z, sibling).wait_send()

        @pl.loop(0, count)
        def _(zz):
            for small in range(2):
                sent = (gathered, gathered_s)[small].at[zz]
                for i in range(2):
                    up = 2 * i - 1

                    @pl.when((up * (z - zz) >= 0) & inside(z + up))
                    def _():
                        copy(
                            sent, sent, zs_send.at[i, small, zz], zs_recv.at[0, zz], z, sibling
                        ).wait_send()

    for k, item in enumerate(item_order):
        if k == out_items // 2:
            drain()
        total_of(z, item)

        def body(i):
            @pl.when(inside(z - (2 * i - 1)))
            def _():
                take_line(i, z, item)

        both(body)
        if item == out_pieces:
            sums_s[z] = acc_s[...].astype(BF16)
            last_move().start()
        elif item > 0:
            expert_ref[:, out_columns[item]] = (
                acc[:, out_columns[item]] + shared[:, out_columns[item]]
            ).astype(BF16)

    for r in (1, 2, 3):
        sent = chosen.at[:, band(r), reach(r, out_cut)]
        copy(sent, sent, xr_send.at[r], xa_recv.at[r, 0], z, sibling).wait_send()

    @pl.loop(0, count)
    def _(zz):
        @pl.when(zz != z)
        def _():
            for small in range(2):
                sent = (sums, sums_s)[small].at[zz]
                copy(sent, sent, rz_send.at[small, zz], zs_recv.at[0, zz], z, sibling).wait_send()

    mixer_pair(1).wait_recv()
    mixer_move().wait_recv()
    mixer_ref[...] = (
        terms[0].astype(F32) + mixer_in[1].astype(F32) + mixer_side[...].astype(F32)
    ).astype(BF16)
    last_move().wait_recv()
    expert_ref[:, out_columns[0]] = (
        acc[:, out_columns[0]] + from_side[...].astype(F32) + shared[:, out_columns[0]]
    ).astype(BF16)
    mixer_move().wait_send()
    last_move().wait_send()


def piece_columns(width):
    unit = width // 16
    gather, result = ((0, 2, 5, 8, 10, 12, 14, 16), (0, 3, 5, 8, 10, 12, 14, 16))
    return tuple(
        [slice(a * unit, b * unit) for a, b in zip(edges, edges[1:])] for edges in (gather, result)
    )


def layer(
    queries,
    key_value,
    key_bias,
    out_weight,
    expert_input,
    norm_gain,
    routes,
    route_weights,
    routed_parts,
    shared_parts,
    capacity,
):
    tokens, width = expert_input.shape
    count = lax.axis_size("ep")
    columns, out_columns = piece_columns(width)
    cut, out_cut = columns[0].stop, out_columns[0].stop
    items, out_items = len(columns) + 1, len(out_columns) + 1
    span, _, pair_width = key_value.shape
    head_dim = pair_width // 2
    heads = queries.shape[1] // head_dim
    size = min(span, 256)
    hidden = routed_parts[0].shape[1]
    band = 4 * capacity
    dma = pltpu.SemaphoreType.DMA
    vmem = pl.BlockSpec(memory_space=pltpu.VMEM)
    hbm = pl.BlockSpec(memory_space=pl.ANY)
    buffers = [
        ((count, tokens, width), BF16),
        ((count, tokens, cut), BF16),
        ((count, 8, tokens), F32),
        ((2, count, 8, tokens), F32),
        ((count, 3 * capacity, width), BF16),
        ((count, capacity, cut), BF16),
        ((count, band, width), BF16),
        ((count, band, width), BF16),
        ((count, 2 * capacity, out_cut), BF16),
        ((count, tokens, width), BF16),
        ((count, tokens, out_cut), BF16),
        ((2, count, tokens, width), BF16),
        ((2, count, tokens, out_cut), BF16),
        ((tokens, width), F32),
        ((tokens, out_cut), F32),
        ((tokens, out_cut), BF16),
        ((tokens, width), F32),
        (out_weight.shape, BF16),
        (shared_parts[0].shape, BF16),
        (shared_parts[1].shape, BF16),
        (shared_parts[2].shape, BF16),
        ((width, hidden), BF16),
        ((width, hidden), BF16),
        ((hidden, width), BF16),
        ((span, pair_width), BF16),
        ((8, span), F32),
        ((8, span), F32),
        ((2, head_dim, span), BF16),
        ((2, span, 128), F32),
        ((heads, span // size, head_dim, size), F32),
        ((heads, span // size, 8, size), F32),
        ((heads * head_dim, span), BF16),
        ((4, tokens, width), BF16),
        ((2, tokens, width), BF16),
        ((tokens, width), BF16),
        ((tokens, width), BF16),
    ]
    semaphores = [
        (7,),
        (2, count),
        (2, count),
        (2,),
        (2,),
        (2, 2, count),
        (items, count),
        (1,),
        (1,),
        (4,),
        (4, count),
        (4,),
        (4, out_items - 1, count),
        (2, count),
        (2, out_items, count),
        (1,),
        (1,),
        (3,),
        (3,),
    ]
    return pl.pallas_call(
        lambda *refs: layer_kernel(capacity, *refs),
        out_shape=[pltpu.VMEM((tokens, width), BF16)] * 2,
        in_specs=[vmem] * 7 + [hbm] * 7,
        out_specs=[vmem] * 2,
        scratch_shapes=[pltpu.VMEM(*b) for b in buffers] + [dma(s) for s in semaphores],
        compiler_params=pltpu.CompilerParams(
            collective_id=0, has_side_effects=True, vmem_limit_bytes=60 * 2**20
        ),
        name="layer",
        cost_estimate=pl.CostEstimate(flops=10**10, bytes_accessed=2 * 10**7, transcendentals=0),
    )(
        queries.T,
        key_value.reshape(span, pair_width),
        key_bias,
        expert_input,
        norm_gain.reshape(1, width),
        routes.T,
        route_weights.T,
        out_weight,
        *shared_parts,
        *routed_parts,
    )


def expert_rows(arrived, gate_weight, up_weight, down_weight):
    sources, capacity, model_width = arrived.shape
    flat_rows = arrived.reshape(sources * capacity, model_width)
    gate_part = jnp.dot(flat_rows, gate_weight[0], preferred_element_type=jnp.float32)
    up_part = jnp.dot(flat_rows, up_weight[0], preferred_element_type=jnp.float32)
    hidden = (jax.nn.silu(gate_part) * up_part).astype(jnp.bfloat16)
    result = jnp.dot(hidden, down_weight[0], preferred_element_type=jnp.float32).astype(
        jnp.bfloat16
    )
    return result.reshape(sources, capacity, model_width)


def experts_half(
    expert_input,
    norm_gain,
    routes,
    route_weights,
    gate_weight,
    up_weight,
    down_weight,
    shared_gate,
    shared_up,
    shared_down,
):
    tokens, top_count = routes.shape
    model_width = expert_input.shape[1]
    ep_count = lax.axis_size("ep")
    tp_count = lax.axis_size("tp")
    experts = ep_count * tp_count
    capacity = max(2, 3 * tokens * top_count // (2 * experts))
    widened = expert_input.astype(jnp.float32)
    normed = (
        widened * lax.rsqrt(jnp.mean(widened * widened, axis=-1, keepdims=True) + 1e-06) * norm_gain
    ).astype(jnp.bfloat16)
    flat_routes = routes.reshape(-1)
    one_hot = (flat_routes[:, None] == jnp.arange(experts, dtype=jnp.int32)[None, :]).astype(
        jnp.int32
    )
    before = jnp.cumsum(one_hot, axis=0) - one_hot
    slot_index = jnp.sum(before * one_hot, axis=1)
    target = flat_routes * capacity + slot_index
    picker = (jnp.arange(experts * capacity, dtype=jnp.int32)[:, None] == target[None, :]).astype(
        jnp.bfloat16
    )
    picker = jnp.sum(picker.reshape(experts * capacity, tokens, top_count), axis=2)
    outgoing = jnp.dot(picker, normed, preferred_element_type=jnp.float32).astype(jnp.bfloat16)
    outgoing = outgoing.reshape(experts, capacity, model_width)
    came_back = lax.all_to_all(
        expert_rows(
            lax.all_to_all(outgoing, ("ep", "tp"), split_axis=0, concat_axis=0, tiled=True),
            gate_weight,
            up_weight,
            down_weight,
        ),
        ("ep", "tp"),
        split_axis=0,
        concat_axis=0,
        tiled=True,
    )
    back_rows = came_back.reshape(experts * capacity, model_width)
    picked = jnp.take(back_rows, target, axis=0).reshape(tokens, top_count, model_width)
    routed = jnp.sum(picked.astype(jnp.float32) * route_weights[:, :, None], axis=1)
    shared_hidden = (
        jax.nn.silu(jnp.dot(normed, shared_gate, preferred_element_type=jnp.float32))
        * jnp.dot(normed, shared_up, preferred_element_type=jnp.float32)
    ).astype(jnp.bfloat16)
    shared_term = jnp.dot(shared_hidden, shared_down, preferred_element_type=jnp.float32)
    return (routed + shared_term).astype(jnp.bfloat16)


def per_device(
    queries,
    key_value,
    key_bias,
    out_weight,
    expert_input,
    norm_gain,
    routes,
    route_weights,
    gate_weight,
    up_weight,
    down_weight,
    shared_gate,
    shared_up,
    shared_down,
):
    tokens, top_count = routes.shape
    span, key_groups, pair_width = key_value.shape
    width = expert_input.shape[1]
    ep_count, tp_count = lax.axis_size("ep"), lax.axis_size("tp")
    experts = ep_count * tp_count
    capacity = max(2, 3 * tokens * top_count // (2 * experts))
    fits = experts * tokens * width * 2 <= 8 * 2**20 and capacity % 16 == 0 and ep_count >= 3
    whole = tp_count == 4 and span == tp_count * tokens and tokens == 128
    heads_fit = key_groups == 1 and pair_width == 128 and width % 1024 == 0
    if fits and whole and heads_fit and furthest_place(ep_count) <= 1:
        return tuple(
            layer(
                queries,
                key_value,
                key_bias,
                out_weight,
                expert_input,
                norm_gain,
                routes,
                route_weights,
                (gate_weight[0], up_weight[0], down_weight[0]),
                (shared_gate, shared_up, shared_down),
                capacity,
            )
        )
    terms = project(attend(queries, key_value, key_bias), out_weight)
    mixer_output = lax.psum_scatter(terms, "tp", scatter_dimension=0, tiled=True)
    expert_output = experts_half(
        expert_input,
        norm_gain,
        routes,
        route_weights,
        gate_weight,
        up_weight,
        down_weight,
        shared_gate,
        shared_up,
        shared_down,
    )
    return (mixer_output, expert_output)


def solution(mesh):
    placed = (
        P(("grp", "ep"), "tp"),
        P(("grp", "ep"), "tp", None),
        P("tp", ("grp", "ep")),
        P("tp", None),
        P(("grp", "ep", "tp"), None),
        P(),
        P(("grp", "ep", "tp"), None),
        P(("grp", "ep", "tp"), None),
        P(("ep", "tp"), None, None),
        P(("ep", "tp"), None, None),
        P(("ep", "tp"), None, None),
        P(),
        P(),
        P(),
    )
    return jax.shard_map(
        per_device,
        mesh=mesh,
        in_specs=placed,
        out_specs=(P(("grp", "ep", "tp"), None), P(("grp", "ep", "tp"), None)),
        check_vma=False,
    )
```
